32 devices in a mesh: ep: 8 (over z, y), tp: 4 (over x, core).
Axes of the slice: x: 2, y: 2, z: 4, core: 2. Of those that a mesh axis runs over, the one named last changes fastest.
Arguments:
- tokens: bfloat16 [1024, 2048], P('ep'), may hold values from -6 to 6
- cotangent: bfloat16 [1024, 2048], P('ep'), may hold values from -6 to 6
- routing: int32 [1024, 2], P('ep'), may hold values from 0 to 7, all different within a row; in each aligned block of 128 rows (0 to 127, 128 to 255, ...) at most 64 rows name the same one
- router_weight: bfloat16 [2048, 8], replicated, may hold values from -0.125 to 0.125
- gate_weight: bfloat16 [8, 2048, 512], P('ep', None, 'tp'), may hold values from -0.125 to 0.125
- up_weight: bfloat16 [8, 2048, 512], P('ep', None, 'tp'), may hold values from -0.125 to 0.125
- down_weight: bfloat16 [8, 512, 2048], P('ep', 'tp'), may hold values from -0.25 to 0.25
Outputs:
- grad_tokens: bfloat16 [1024, 2048], P('ep', 'tp')
- grad_gating: float32 [1024, 2], P('ep')
- grad_router: float32 [2048, 8], P('ep')
- grad_gate_weight: bfloat16 [8, 2048, 512], P('ep', None, 'tp')
- grad_up_weight: bfloat16 [8, 2048, 512], P('ep', None, 'tp')
- grad_down_weight: bfloat16 [8, 512, 2048], P('ep', 'tp')
- in_norms: float32 [8, 2, 2048], P('ep')
- down_norms: float32 [8, 512], P('ep', 'tp')
- router_norms: float32 [2048], P('ep')
The draws below stay inside these ranges and needn't reach their ends.
Inputs may be any that keep to these rules, and one draw needn't show every extreme that they name: `routing`: each row names 2 different experts. Among the rows of one index of ep no expert is named by more than 64 rows, a bound that some block reaches in some of them.
All inputs are finite; a program needn't handle non-finite values.
Results may differ from the reference program's by a relative error of at most 0.014.
Values may be sent and summed in bfloat16 or wider, within the bound.
A program may use at most 64 MiB of HBM per device.

```python
import math
import jax
import jax.numpy as jnp
import numpy as np
from jax import lax

D = 2048
F = 512
TOP = 2
TOK_DEV = 128
EXPERTS = 8
TOKENS = 1024
CAP = 64
N_EP = 8
N_TP = 4


def raised(values, rng, source, target, shards_of, factor):
    owner, partner = [(jnp.arange(values.shape[dim]) // (values.shape[dim] // shards_of)).reshape([-1 if axis == dim else 1 for axis in range(values.ndim)]) for dim in (source, target)]
    chosen = jax.random.permutation(rng, shards_of)[partner]
    strong = (owner == chosen) | (owner == (partner + shards_of // 2) % shards_of)
    return jnp.where(strong, factor * values, values)


def level_of(stream_key, shape, pieces, smallest, largest):
    def one(dim, shards_of):
        heights = jax.random.uniform(jax.random.fold_in(jax.random.fold_in(stream_key, 6), dim), (shards_of,), jnp.float32, smallest / len(pieces), largest / len(pieces))
        return jnp.repeat(jnp.exp(heights), shape[dim] // shards_of).reshape((-1,) + (1,) * (len(shape) - dim - 1))

    level = one(*pieces[0])
    for cut in pieces[1:]:
        level = level * one(*cut)
    return level


def routed_block(stream_key, own, number, rows, number_of, top, bound, slope):
    ranking = jax.random.permutation(stream_key, number_of)
    packed, usual = shares(number_of, rows * top, bound, slope, True), shares(number_of, rows * top, bound, slope, False)
    places = jnp.arange(number_of)

    def named(sizes, turn):
        used = int((sizes > 0).sum())
        fixed = max(1, used // 4)
        shifted = fixed + (places - fixed + turn * (used - fixed)) % max(1, number_of - fixed)
        return jnp.zeros((number_of,), jnp.int32).at[ranking[jnp.where(places < fixed, places, shifted)]].set(jnp.asarray(sizes, jnp.int32))

    sizes = jnp.where(number % 4 == 0, named(packed, number // 4), named(usual, number - number // 4 - 1))
    mixed = jax.random.permutation(jax.random.fold_in(own, 3), number_of)
    donor, receiver = mixed[0:number_of // 2 * 2:2], mixed[1:number_of // 2 * 2:2]
    room = jnp.minimum(sizes[donor] - 1, bound - sizes[receiver]) // 2
    room = jnp.where((donor == ranking[0]) | (receiver == ranking[0]) | (sizes[receiver] == 0), 0, jnp.maximum(room, 0))
    shifted = jax.random.randint(jax.random.fold_in(own, 4), (number_of // 2,), 0, 1 << 20) % (room + 1)
    sizes = sizes.at[donor].add(-shifted).at[receiver].add(shifted)
    members = jnp.searchsorted(jnp.cumsum(sizes), jnp.arange(rows * top), side="right").astype(jnp.int32)
    listing = members.reshape(top, rows).T
    listing = listing[jax.random.permutation(jax.random.fold_in(own, 1), rows)]
    turn = jax.random.randint(jax.random.fold_in(own, 2), (rows, 1), 0, top)
    return jnp.take_along_axis(listing, (jnp.arange(top)[None, :] + turn) % top, axis=1)


def shares(count, total, limit, slope, full):
    portions = [(1 << 20) // math.isqrt(rank ** slope) + 1 for rank in range(1, count + 1)]
    largest = limit if full else min(limit, max(-(-total // count), total * portions[0] // sum(portions)))
    least = 1 if total - largest >= count - 1 else 0
    counts, surplus = [largest] + [least] * (count - 1), total - largest - least * (count - 1)
    while surplus > 0:
        movable = [i for i in range(1, count) if counts[i] < largest] or [i for i in range(1, count) if counts[i] < limit]
        whole, budget = sum([portions[i] for i in movable]), surplus
        for i in movable:
            addition = min(limit - counts[i], max(1, budget * portions[i] // whole), surplus)
            counts[i] = counts[i] + addition
            surplus = surplus - addition
    return np.array(counts)


def centred(stream_key, extent, scale, bound, cuts=(), held_as=jnp.bfloat16):
    values = scale * jax.random.normal(stream_key, extent, jnp.float32)
    if cuts:
        values = values * level_of(stream_key, extent, cuts, -0.22, 0.18)
    return jnp.clip(values, -bound, bound).astype(held_as)


def gaussian_with(own_key, extent, scale, reach, split, heavy, held_as=jnp.bfloat16):
    drawn = scale * jax.random.normal(own_key, extent, jnp.float32)
    if split:
        drawn = drawn * level_of(own_key, extent, split, -0.22, 0.18)
    return jnp.clip(raised(drawn, jax.random.fold_in(own_key, 3), *heavy), -reach, reach).astype(held_as)


def setup_inputs(seed: int = 0) -> dict:
    arg_keys = jax.random.split(jax.random.key(seed), 8)
    tokens = gaussian_with(arg_keys[0], (TOKENS, D), 1.0, 6.0, ((0, 8),), (0, 1, 8, 2.0))
    cotangent = centred(arg_keys[1], (TOKENS, D), 1.0, 6.0, ((0, 8),))
    routing_keys = jax.random.split(jax.random.fold_in(arg_keys[2], 1), TOKENS // TOK_DEV)
    routing_turns = jax.random.permutation(jax.random.fold_in(arg_keys[2], 3), TOKENS // TOK_DEV)
    routing = jax.vmap(lambda own, number: routed_block(jax.random.fold_in(arg_keys[2], 2), own, number, TOK_DEV, EXPERTS, TOP, CAP, 2))(routing_keys, routing_turns).reshape((TOKENS, TOP))
    router_weight = centred(arg_keys[3], (D, EXPERTS), D ** -0.5, 0.125)
    gate_weight = centred(arg_keys[4], (EXPERTS, D, F), D ** -0.5, 0.125, ((0, 8), (2, 4)))
    up_weight = centred(arg_keys[5], (EXPERTS, D, F), D ** -0.5, 0.125, ((0, 8), (2, 4)))
    down_weight = centred(arg_keys[6], (EXPERTS, F, D), F ** -0.5, 0.25, ((0, 8), (1, 4)))
    return {"tokens": tokens, "cotangent": cotangent, "routing": routing, "router_weight": router_weight, "gate_weight": gate_weight, "up_weight": up_weight, "down_weight": down_weight}


def silu_parts(pre_gate):
    sigmoid_gate = jax.nn.sigmoid(pre_gate)
    return pre_gate * sigmoid_gate, sigmoid_gate * (1.0 + pre_gate * (1.0 - sigmoid_gate))


def block_layout(block_routing):
    flat_expert = block_routing.reshape(-1)
    one_hot = (flat_expert[:, None] == jnp.arange(EXPERTS, dtype=jnp.int32)[None, :]).astype(jnp.int32)
    earlier = jnp.cumsum(one_hot, axis=0) - one_hot
    within = jnp.sum(earlier * one_hot, axis=1)
    position = (flat_expert * CAP + within).astype(jnp.int32)
    vacant = jnp.full((EXPERTS * CAP,), -1, jnp.int32)
    return vacant.at[position].set(jnp.arange(TOK_DEV * TOP, dtype=jnp.int32))


def reference(tokens, cotangent, routing, router_weight, gate_weight, up_weight, down_weight):
    local_layout = jax.vmap(block_layout)(routing.reshape(N_EP, TOK_DEV, TOP))
    offsets = (jnp.arange(N_EP, dtype=jnp.int32) * (TOK_DEV * TOP))[:, None]
    global_layout = jnp.where(local_layout >= 0, local_layout + offsets, TOKENS * TOP).astype(jnp.int32)
    expert_layout = global_layout.reshape(N_EP, EXPERTS, CAP).transpose(1, 0, 2).reshape(EXPERTS, N_EP * CAP)

    logits = jnp.dot(tokens, router_weight, preferred_element_type=jnp.float32)
    scores = jax.nn.sigmoid(jnp.take_along_axis(logits, routing, axis=1))
    score_sum = jnp.sum(scores, axis=1, keepdims=True)
    gating = scores / score_sum
    flat_gating = jnp.concatenate([gating.reshape(-1), jnp.zeros((1,), jnp.float32)])
    padded_tokens = jnp.concatenate([tokens, jnp.zeros((1, D), jnp.bfloat16)], axis=0)
    padded_cotangent = jnp.concatenate([cotangent, jnp.zeros((1, D), jnp.bfloat16)], axis=0)
    hidden_block = F // N_TP
    arrived = N_EP * CAP

    def one_expert(carried, inputs):
        token_terms, gating_grads = carried
        slot_layout, weight_gate, weight_up, weight_down = inputs
        source_rows = slot_layout // TOP
        rows_in = padded_tokens[source_rows]
        cot_rows = padded_cotangent[source_rows]
        slot_gating = flat_gating[slot_layout][:, None]
        pre_gate = jnp.dot(rows_in, weight_gate, preferred_element_type=jnp.float32)
        pre_up = jnp.dot(rows_in, weight_up, preferred_element_type=jnp.float32)
        activated, silu_slope = silu_parts(pre_gate)
        hidden = (activated * pre_up).astype(jnp.bfloat16)
        back_raw = lax.dot_general(cot_rows, weight_down, (((1,), (1,)), ((), ())),
                                   preferred_element_type=jnp.float32)
        hidden_wide = hidden.astype(jnp.float32)
        gate_grad = jnp.sum(hidden_wide * back_raw, axis=1)
        scaled_back = slot_gating * back_raw
        grad_pre_gate = (scaled_back * pre_up * silu_slope).astype(jnp.bfloat16)
        grad_pre_up = (scaled_back * activated).astype(jnp.bfloat16)
        scaled_hidden = (slot_gating * hidden_wide).astype(jnp.bfloat16)
        gate_sum = jnp.dot(rows_in.T, grad_pre_gate, preferred_element_type=jnp.float32)
        up_sum = jnp.dot(rows_in.T, grad_pre_up, preferred_element_type=jnp.float32)
        down_sum = jnp.dot(scaled_hidden.T, cot_rows, preferred_element_type=jnp.float32)
        norms_in = jnp.stack([jnp.sum(gate_sum * gate_sum, axis=1), jnp.sum(up_sum * up_sum, axis=1)])
        norms_down = jnp.sum(down_sum * down_sum, axis=1)
        pieces_gate = grad_pre_gate.reshape(arrived, N_TP, hidden_block).astype(jnp.float32)
        pieces_up = grad_pre_up.reshape(arrived, N_TP, hidden_block).astype(jnp.float32)
        blocks_gate = weight_gate.reshape(D, N_TP, hidden_block).astype(jnp.float32)
        blocks_up = weight_up.reshape(D, N_TP, hidden_block).astype(jnp.float32)
        partial_value = (jnp.einsum("rpf,dpf->prd", pieces_gate, blocks_gate)
                   + jnp.einsum("rpf,dpf->prd", pieces_up, blocks_up))
        rounded = lax.optimization_barrier(partial_value.astype(jnp.bfloat16))
        token_term = jnp.sum(rounded.astype(jnp.float32), axis=0).astype(jnp.bfloat16)
        token_terms = token_terms.at[slot_layout].set(token_term)
        gating_grads = gating_grads.at[slot_layout].set(gate_grad)
        return (token_terms, gating_grads), (gate_sum.astype(jnp.bfloat16), up_sum.astype(jnp.bfloat16),
                                             down_sum.astype(jnp.bfloat16), norms_in, norms_down)

    start_terms = jnp.zeros((TOKENS * TOP + 1, D), jnp.bfloat16)
    start_grads = jnp.zeros((TOKENS * TOP + 1,), jnp.float32)
    (token_terms, gating_grads), stacked = lax.scan(
        one_expert, (start_terms, start_grads), (expert_layout, gate_weight, up_weight, down_weight))
    grad_gate_weight, grad_up_weight, grad_down_weight, in_norms, down_norms = stacked

    summed_terms = jnp.sum(token_terms[:TOKENS * TOP].reshape(TOKENS, TOP, D).astype(jnp.float32), axis=1)
    grad_gating = gating_grads[:TOKENS * TOP].reshape(TOKENS, TOP)
    weighted = jnp.sum(gating * grad_gating, axis=1, keepdims=True)
    grad_scores = (grad_gating - weighted) / score_sum
    grad_chosen = grad_scores * scores * (1.0 - scores)
    token_index = jnp.arange(TOKENS, dtype=jnp.int32)[:, None]
    grad_logits = jnp.zeros((TOKENS, EXPERTS), jnp.float32).at[token_index, routing].add(grad_chosen)
    grad_logits = grad_logits.astype(jnp.bfloat16)
    router_term = lax.dot_general(grad_logits, router_weight, (((1,), (1,)), ((), ())),
                                  preferred_element_type=jnp.float32)
    grad_tokens = (summed_terms + router_term).astype(jnp.bfloat16)
    grad_router = jnp.dot(tokens.T, grad_logits, preferred_element_type=jnp.float32)
    router_norms = jnp.sum(grad_router * grad_router, axis=1)
    return (grad_tokens, grad_gating, grad_router, grad_gate_weight, grad_up_weight, grad_down_weight,
            in_norms, down_norms, router_norms)
```

```python
import functools

import jax
import jax.numpy as jnp
from jax import lax
from jax.experimental import pallas as pl
from jax.experimental.pallas import tpu as pltpu
from jax.sharding import PartitionSpec as P


def silu_parts(pre_gate):
    sigmoid_gate = jax.nn.sigmoid(pre_gate)
    return (pre_gate * sigmoid_gate, sigmoid_gate * (1.0 + pre_gate * (1.0 - sigmoid_gate)))


def slot_layout(routing, experts_all, capacity):
    tok_count, top_count = routing.shape
    flat_expert = routing.reshape(-1)
    one_hot = (flat_expert[:, None] == jnp.arange(experts_all, dtype=jnp.int32)[None, :]).astype(
        jnp.int32
    )
    earlier = jnp.cumsum(one_hot, axis=0) - one_hot
    within = jnp.sum(earlier * one_hot, axis=1)
    position = flat_expert * capacity + within
    vacant = jnp.full((experts_all * capacity,), tok_count * top_count, jnp.int32)
    return (vacant.at[position].set(jnp.arange(tok_count * top_count, dtype=jnp.int32)), position)


def general(tokens, cotangent, routing, router_weight, gate_weight, up_weight, down_weight):
    tok_count, model_width = tokens.shape
    top_count = routing.shape[1]
    experts_all = router_weight.shape[1]
    expert_local = gate_weight.shape[0]
    ep_size = lax.axis_size("ep")
    tp_size = lax.axis_size("tp")
    tp_index = lax.axis_index("tp")
    slice_width = model_width // tp_size
    capacity = max(2, 2 * tok_count * top_count // experts_all)
    arrived = ep_size * capacity
    logits = jnp.dot(tokens, router_weight, preferred_element_type=jnp.float32)
    picked = (
        routing[:, :, None] == jnp.arange(experts_all, dtype=jnp.int32)[None, None, :]
    ).astype(jnp.float32)
    scores = jax.nn.sigmoid(jnp.einsum("tke,te->tk", picked, logits))
    score_sum = jnp.sum(scores, axis=1, keepdims=True)
    gating = scores / score_sum
    assignment, position = slot_layout(routing, experts_all, capacity)
    source_row = assignment // top_count
    padded_tokens = jnp.concatenate([tokens, jnp.zeros((1, model_width), tokens.dtype)], axis=0)
    padded_cotangent = jnp.concatenate(
        [cotangent, jnp.zeros((1, model_width), cotangent.dtype)], axis=0
    )
    padded_gating = jnp.concatenate([gating.reshape(-1), jnp.zeros((1,), jnp.float32)])
    sent_gating = padded_gating[assignment].reshape(experts_all, capacity)
    own_tokens = lax.dynamic_slice_in_dim(padded_tokens, tp_index * slice_width, slice_width, 1)
    own_cotangent = lax.dynamic_slice_in_dim(
        padded_cotangent, tp_index * slice_width, slice_width, 1
    )
    part_tokens, part_cotangent = (
        lax.all_to_all(
            own_tokens[source_row].reshape(experts_all, capacity, slice_width),
            "ep",
            split_axis=0,
            concat_axis=0,
            tiled=True,
        ),
        lax.all_to_all(
            own_cotangent[source_row].reshape(experts_all, capacity, slice_width),
            "ep",
            split_axis=0,
            concat_axis=0,
            tiled=True,
        ),
    )
    got_tokens, got_cotangent = (
        lax.all_gather(part_tokens, "tp", axis=2, tiled=True),
        lax.all_gather(part_cotangent, "tp", axis=2, tiled=True),
    )
    got_gating = lax.all_to_all(sent_gating, "ep", split_axis=0, concat_axis=0, tiled=True)

    def by_expert(values):
        shaped = values.reshape((ep_size, expert_local) + values.shape[1:])
        return jnp.moveaxis(shaped, 1, 0).reshape((expert_local, arrived) + values.shape[2:])

    def by_source(values):
        shaped = values.reshape((expert_local, ep_size, capacity) + values.shape[2:])
        return jnp.moveaxis(shaped, 1, 0).reshape(
            (ep_size * expert_local, capacity) + values.shape[2:]
        )

    rows_in = by_expert(got_tokens)
    cot_rows = by_expert(got_cotangent)
    slot_gating = by_expert(got_gating)[:, :, None]
    pre_gate = jnp.einsum("lrd,ldf->lrf", rows_in, gate_weight, preferred_element_type=jnp.float32)
    pre_up = jnp.einsum("lrd,ldf->lrf", rows_in, up_weight, preferred_element_type=jnp.float32)
    activated, silu_slope = silu_parts(pre_gate)
    hidden = (activated * pre_up).astype(jnp.bfloat16)
    back_raw = jnp.einsum("lrd,lfd->lrf", cot_rows, down_weight, preferred_element_type=jnp.float32)
    hidden_wide = hidden.astype(jnp.float32)
    gate_partial = jnp.sum(hidden_wide * back_raw, axis=2)
    scaled_back = slot_gating * back_raw
    grad_pre_gate = (scaled_back * pre_up * silu_slope).astype(jnp.bfloat16)
    grad_pre_up = (scaled_back * activated).astype(jnp.bfloat16)
    scaled_hidden = (slot_gating * hidden_wide).astype(jnp.bfloat16)
    gate_sum = jnp.einsum(
        "lrd,lrf->ldf", rows_in, grad_pre_gate, preferred_element_type=jnp.float32
    )
    up_sum = jnp.einsum("lrd,lrf->ldf", rows_in, grad_pre_up, preferred_element_type=jnp.float32)
    down_sum = jnp.einsum(
        "lrf,lrd->lfd", scaled_hidden, cot_rows, preferred_element_type=jnp.float32
    )
    down_norms = jnp.sum(down_sum * down_sum, axis=2)
    back_partial = jnp.einsum(
        "lrf,ldf->lrd", grad_pre_gate, gate_weight, preferred_element_type=jnp.float32
    ) + jnp.einsum("lrf,ldf->lrd", grad_pre_up, up_weight, preferred_element_type=jnp.float32)
    back_rounded = back_partial.astype(jnp.bfloat16)
    slot_values = (
        lax.psum_scatter(back_rounded, "tp", scatter_dimension=2, tiled=True)
        .astype(jnp.float32)
        .astype(jnp.bfloat16)
    )
    gating_total, gate_rows, up_rows = lax.psum(
        (gate_partial, jnp.sum(gate_sum * gate_sum, axis=2), jnp.sum(up_sum * up_sum, axis=2)), "tp"
    )
    home_values = lax.all_to_all(
        by_source(slot_values), "ep", split_axis=0, concat_axis=0, tiled=True
    )
    home_gating = lax.all_to_all(
        by_source(gating_total), "ep", split_axis=0, concat_axis=0, tiled=True
    )
    flat_values = home_values.reshape(experts_all * capacity, slice_width)
    token_terms = (
        flat_values[position].reshape(tok_count, top_count, slice_width).astype(jnp.float32)
    )
    grad_gating = home_gating.reshape(-1)[position].reshape(tok_count, top_count)
    weighted = jnp.sum(gating * grad_gating, axis=1, keepdims=True)
    grad_scores = (grad_gating - weighted) / score_sum
    grad_chosen = grad_scores * scores * (1.0 - scores)
    grad_logits = jnp.einsum("tk,tke->te", grad_chosen, picked).astype(jnp.bfloat16)
    router_slice = lax.dynamic_slice_in_dim(router_weight, tp_index * slice_width, slice_width, 0)
    router_term = jnp.einsum(
        "te,de->td", grad_logits, router_slice, preferred_element_type=jnp.float32
    )
    grad_tokens = (jnp.sum(token_terms, axis=1) + router_term).astype(jnp.bfloat16)
    grad_router = lax.psum_scatter(
        jnp.einsum("td,te->de", tokens, grad_logits, preferred_element_type=jnp.float32),
        "ep",
        scatter_dimension=0,
        tiled=True,
    )
    router_norms = jnp.sum(grad_router * grad_router, axis=1)
    in_norms = jnp.stack([gate_rows, up_rows], axis=1)
    return (
        grad_tokens,
        grad_gating,
        grad_router,
        gate_sum.astype(jnp.bfloat16),
        up_sum.astype(jnp.bfloat16),
        down_sum.astype(jnp.bfloat16),
        in_norms,
        down_norms,
        router_norms,
    )


MESH = pl.DeviceIdType.MESH
F32 = jnp.float32
BF16 = jnp.bfloat16


def contract(a, b, dims, precision=None):
    return lax.dot_general(
        a, b, ((dims[0], dims[1]), ((), ())), precision=precision, preferred_element_type=F32
    )


def flipped(index, mask, bits):
    out = index
    for bit in range(bits):
        if (mask >> bit) & 1:
            out = out + (1 << bit) * (1 - 2 * ((index // (1 << bit)) % 2))
    return out


def kernel(n_ep, n_tp, cap,
           tok_hbm, cot_hbm, rt_hbm, rw_hbm, wg, wu, wd_hbm,
           o_tok, o_gg, o_gr, o_gate, o_up, o_down, o_norm, o_dnorm, o_rnorm,
           rt, rw, tok, cot, wgu, wd, sel, raw, info, other_x, ysa, ysx, arr_a, gs, gr, part, pc, xs, xr,
           fin, home, gp, sh, ggb, ggc, ggx, ggh, nb, nc, nx, rp, rr, lsem, ssem, rsem):
    e = lax.axis_index("ep")
    p = lax.axis_index("tp")
    n_z = n_ep // 2
    z, y = e // 2, e % 2
    toks, width = tok.shape
    n_exp = rw.shape[0]
    fb = width // n_tp
    hid = wd.shape[0]
    two = 2 * cap
    pieces = [(arr_a, b, b * fb, fb) for b in range(n_tp)]
    p_core, p_x, p_both = (flipped(p, m, 2) for m in (1, 2, 3))
    started, local = [], []

    def ep_at(d, h=0):
        return ((z + d) % n_z) * 2 + (y + h) % 2

    def send(source, dest, ep=None, tp=None):
        i = len(started)
        copy = pltpu.make_async_remote_copy(
            src_ref=source, dst_ref=dest, send_sem=ssem.at[i], recv_sem=rsem.at[i],
            device_id=(e if ep is None else ep, p if tp is None else tp), device_id_type=MESH)
        copy.start()
        started.append(copy)
        return copy

    def load(source, dest):
        copy = pltpu.make_async_copy(source, dest, lsem.at[len(local)])
        copy.start()
        local.append(copy)
        return copy

    barrier = pltpu.get_barrier_semaphore()
    offsets = [(0, 1)] + [(d, h) for d in (2, 1, 3) for h in (0, 1)]
    for d, h in offsets:
        pl.semaphore_signal(barrier, inc=1, device_id=(ep_at(d, h), p), device_id_type=MESH)
    for other in (p_core, p_x):
        pl.semaphore_signal(barrier, inc=1, device_id=(e, other), device_id_type=MESH)
    routing_in = load(rt_hbm, rt)
    cols = pl.ds(pl.multiple_of(p * fb, 128), fb)
    cols_x = pl.ds(pl.multiple_of(p_x * fb, 128), fb)
    raw_in = [load(tok_hbm.at[:, cols], raw.at[0, 0]), load(cot_hbm.at[:, cols], raw.at[0, 1])]
    raw_in += [load(tok_hbm.at[:, cols_x], other_x.at[0]), load(cot_hbm.at[:, cols_x], other_x.at[1])]
    full_in = [load(rw_hbm, rw), load(tok_hbm, tok), load(cot_hbm, cot)]
    weights_in = [load(wg, wgu.at[:, pl.ds(0, hid)]), load(wu, wgu.at[:, pl.ds(hid, hid)]),
                  load(wd_hbm, wd)]

    routing_in.wait()
    r0, r1 = rt[0:1, :], rt[1:2, :]
    row_e = lax.broadcasted_iota(jnp.int32, (128, toks), 0)
    member_t = (r0 == row_e) | (r1 == row_e)
    earlier = (lax.broadcasted_iota(jnp.int32, (toks, toks), 0)
               < lax.broadcasted_iota(jnp.int32, (toks, toks), 1))
    place_t = contract(member_t.astype(F32).astype(BF16), earlier.astype(F32).astype(BF16),
                       ((1,), (0,)))
    place_t = jnp.where(member_t, place_t, -1000.0)
    info[0] = place_t[:n_exp]
    slot_id = lax.broadcasted_iota(jnp.int32, (cap, toks), 0).astype(F32)
    e_y = ep_at(0, 1)

    def chosen(d, x):
        return (info[d, pl.ds(x, 1), :] == slot_id).astype(F32).astype(BF16)

    for copy in raw_in:
        copy.wait()
    pl.semaphore_wait(barrier, n_ep + 1)

    right, left = ep_at(1), ep_at(n_z - 1)
    ring, infos = {}, {}
    for d in (1, 3, 2):
        infos[n_z - d] = send(info.at[0], info.at[n_z - d], ep=ep_at(d))
    for a in (0, 1):
        ring[3, a] = send(raw.at[0, a], raw.at[3, a], ep=right)
    for a in (0, 1):
        ring[1, a] = send(raw.at[0, a], raw.at[1, a], ep=left)

    to_y, xed, cored, cored2 = {}, {}, {}, {}

    def spread(src, a, key):
        xed[key, a] = send(arr_a.at[p, src, a], arr_a.at[p, src, a], tp=p_x)

    def pick(d, a):
        src = ep_at(d)
        if d:
            picks = jnp.concatenate([chosen(d, e_y), chosen(d, e)], axis=0)
        else:
            picks = chosen(d, e_y)
            ysx[a] = contract(picks, other_x[a], ((1,), (0,))).astype(BF16)
        rows = contract(picks, raw[d, a], ((1,), (0,))).astype(BF16)
        ysa[d, a] = rows[:cap]
        to_y[d, a] = [send(ysa.at[d, a], arr_a.at[p, src, a], ep=e_y)]
        if d:
            arr_a[p, src, a] = rows[cap:]
            spread(src, a, (d, 0))
        else:
            to_y[d, a].append(send(ysx.at[a], arr_a.at[p_x, src, a], ep=e_y))

    def arrive(d, a):
        ring[d, a].wait_recv()
        if d == 3:
            ring[2, a] = send(raw.at[3, a], raw.at[2, a], ep=right)
        pick(d, a)

    def from_y(d, a):
        for copy in to_y[d, a]:
            copy.wait_recv()
        if d:
            spread(ep_at(d, 1), a, (d, 1))

    def to_core(d, h):
        src = ep_at(d, h)
        cored[d, h] = send(arr_a.at[p, src], arr_a.at[p, src], tp=p_core)

    def x_to_core(d, h):
        if d:
            xed[(d, h), 0].wait_recv()
            xed[(d, h), 1].wait_recv()
        src = ep_at(d, h)
        cored2[d, h] = send(arr_a.at[p_x, src], arr_a.at[p_x, src], tp=p_core)

    pick(0, 0)
    pick(0, 1)

    for copy in full_in:
        copy.wait()
    for x in range(n_exp):
        sel[x] = (place_t[x:x + 1, :] == slot_id).astype(F32).astype(BF16)
    all_sel = sel[...].reshape(n_exp * cap, toks)
    place = jnp.transpose(place_t)
    member8 = place[:, :n_exp] > -1.0
    logits = contract(tok[...], rw[...], ((1,), (1,)))
    score = jnp.where(member8, jax.nn.sigmoid(logits), 0.0)
    score_sum = jnp.sum(score, axis=1, keepdims=True)
    gating = score / score_sum
    lane_s = (lax.broadcasted_iota(jnp.int32, (toks, two), 1) - y * cap).astype(F32)

    def hit(x):
        return (place[:, x:x + 1] == lane_s).astype(F32)

    for x in range(n_exp):
        row = jnp.sum(hit(x) * gating[:, x:x + 1], axis=0, keepdims=True)
        gs[x] = jnp.broadcast_to(row, (8, two))
    gated = {}
    for d, h in offsets:
        other = ep_at(d, h)
        gated[(n_z - d) % n_z, h] = send(gs.at[other], gr.at[e], ep=other)
    gr[e] = gs[e]
    own = sel[e]
    for a, ref in enumerate((tok, cot)):
        rows = contract(own, ref[...], ((1,), (0,))).astype(BF16)
        for ref_b, b, start, size in pieces:
            ref_b[b, e, a] = rows[:, start:start + size]

    ret_c, ret_x, ret_f = {}, {}, {}

    def base_of(q):
        return ((z + q) % n_z) * 2

    def compute(q):
        for h in ((1,) if q == 0 else (0, 1)):
            gated[q, h].wait_recv()
            cored[q, h].wait_recv()
            cored2[q, h].wait_recv()
        base = base_of(q)
        pair = pl.ds(base, 2)
        here = pl.ds(pl.multiple_of(base * cap, two), two)
        pre = jnp.zeros((two, 2 * hid), F32)
        back = jnp.zeros((two, hid), F32)
        for ref_b, b, start, size in pieces:
            c = slice(start, start + size)
            pre = pre + contract(ref_b[b, pair, 0].reshape(two, size), wgu[c, :], ((1,), (0,)))
            back = back + contract(ref_b[b, pair, 1].reshape(two, size), wd[:, c], ((1,), (1,)))
        gate = jnp.transpose(gr[base] + gr[base + 1])[:, 0:1]
        pre_gate, pre_up = pre[:, :hid], pre[:, hid:]
        activated, slope = silu_parts(pre_gate)
        hidden = (activated * pre_up).astype(BF16).astype(F32)
        prod = hidden * back
        ggb[base // 2] = contract(jnp.ones((8, hid), F32), prod, ((1,), (1,)),
                                  lax.Precision.HIGHEST)
        scaled = gate * back
        grads = jnp.concatenate([(scaled * pre_up * slope).astype(BF16),
                                 (scaled * activated).astype(BF16)], axis=1)
        gp[here, :] = grads
        sh[here, :] = (gate * hidden).astype(BF16)
        for b in range(n_tp):
            part[b, pair] = contract(grads, wgu[b * fb:(b + 1) * fb, :], ((1,), (1,))).astype(
                BF16).reshape(2, cap, fb)
        ret_c[q] = (send(part.at[p_both, pair], pc.at[1, pair], tp=p_core),
                    send(part.at[p_core, pair], pc.at[0, pair], tp=p_core))

    def to_x(q):
        pair = pl.ds(base_of(q), 2)
        ret_c[q][0].wait_recv()
        xs[pair] = (part[p_x, pair].astype(F32) + pc[1, pair].astype(F32)).astype(BF16)
        ret_x[q] = send(xs.at[pair], xr.at[pair], tp=p_x)

    def to_home(q):
        pair = pl.ds(base_of(q), 2)
        ret_c[q][1].wait_recv()
        ret_x[q].wait_recv()
        fin[pair] = (part[p, pair].astype(F32) + pc[0, pair].astype(F32)
                     + xr[pair].astype(F32)).astype(BF16)
        for h in ((1,) if q == 0 else (0, 1)):
            other = ep_at(q, h)
            ret_f[q, h] = send(fin.at[other], home.at[e], ep=other)
        if q == 0:
            home[e] = fin[e]

    for d in (3, 1, 2):
        infos[d].wait_recv()
    from_y(0, 0)
    from_y(0, 1)
    to_core(0, 1)
    x_to_core(0, 1)
    arrive(3, 0)
    from_y(3, 0)
    arrive(3, 1)
    to_core(3, 0)
    from_y(3, 1)
    to_core(3, 1)
    for copy in weights_in:
        copy.wait()
    compute(0)
    arrive(1, 0)
    x_to_core(3, 0)
    from_y(1, 0)
    to_x(0)
    arrive(1, 1)
    to_core(1, 0)
    x_to_core(3, 1)
    from_y(1, 1)
    to_core(1, 1)
    compute(3)
    to_home(0)
    arrive(2, 0)
    from_y(2, 0)
    x_to_core(1, 0)
    to_x(3)
    arrive(2, 1)
    to_core(2, 0)
    x_to_core(1, 1)
    from_y(2, 1)
    to_core(2, 1)
    compute(1)
    to_home(3)
    x_to_core(2, 0)
    x_to_core(2, 1)
    to_x(1)
    compute(2)
    last = 2
    gg_c = send(ggb, ggc, tp=p_core)
    to_x(last)
    gg_c.wait_recv()
    ggb2 = ggb[...] + ggc[...]
    ggc[...] = ggb2
    gg_x = send(ggc, ggx, tp=p_x)
    to_home(1)
    grads = gp[...]

    def in_block(i):
        ref_b, b, start, size = pieces[i]
        rows = ref_b[b, :, 0].reshape(n_ep * cap, size)
        sums = contract(grads, rows, ((0,), (0,)))
        c = slice(start, start + size)
        o_gate[c, :] = jnp.transpose(sums[:hid]).astype(BF16)
        o_up[c, :] = jnp.transpose(sums[hid:]).astype(BF16)
        nb[0:1, c] = jnp.sum(sums[:hid] * sums[:hid], axis=0, keepdims=True)
        nb[1:2, c] = jnp.sum(sums[hid:] * sums[hid:], axis=0, keepdims=True)

    in_block(0)
    gg_x.wait_recv()
    ggx[...] = ggb2 + ggx[...]
    gg_f = {}
    for k in offsets:
        other = ep_at(*k)
        gg_f[k] = send(ggx.at[other // 2], ggh.at[e], ep=other)
    ggh[e] = ggx[e // 2]
    in_block(1)
    to_home(last)
    for i in range(2, len(pieces)):
        in_block(i)
    nb_c = send(nb, nc, tp=p_core)

    for k in offsets:
        gg_f[k].wait_recv()
    lane8 = lax.broadcasted_iota(jnp.int32, (toks, n_exp), 1)
    got = jnp.zeros((toks, n_exp), F32)
    for x in range(n_exp):
        col = jnp.sum(hit(x) * ggh[x, 0:1, :], axis=1, keepdims=True)
        got = got + jnp.where(lane8 == x, col, 0.0)
    got_t = jnp.transpose(jnp.concatenate(
        [got, jnp.zeros((toks, 128 - n_exp), F32)], axis=1))[:n_exp]
    for k, r in enumerate((r0, r1)):
        o_gg[k:k + 1, :] = jnp.sum(jnp.where(r == row_e[:n_exp], got_t, 0.0), axis=0, keepdims=True)
    weighted = jnp.sum(gating * got, axis=1, keepdims=True)
    grad_logits = jnp.where(member8, (got - weighted) / score_sum * score * (1.0 - score),
                            0.0).astype(BF16)
    rp[...] = contract(grad_logits, tok[...], ((0,), (0,)))
    span = width // n_ep
    rr_f = {}
    for k in offsets:
        other = ep_at(*k)
        rr_f[k] = send(rp.at[:, pl.ds(pl.multiple_of(other * span, 128), span)], rr.at[e], ep=other)
    rr[e] = rp[:, pl.ds(pl.multiple_of(e * span, 128), span)]
    nb_c.wait_recv()
    nc[...] = nb[...] + nc[...]
    nb_x = send(nc, nx, tp=p_x)
    shv = sh[...]
    dn = jnp.zeros((hid, 1), F32)
    for ref_b, b, start, size in pieces:
        sums = contract(shv, ref_b[b, :, 1].reshape(n_ep * cap, size), ((0,), (0,)))
        o_down[:, start:start + size] = sums.astype(BF16)
        dn = dn + jnp.sum(sums * sums, axis=1, keepdims=True)
    o_dnorm[...] = jnp.transpose(jnp.broadcast_to(dn, (hid, 128)))[0:1, :]
    router_term = contract(grad_logits, rw[:, cols], ((1,), (0,)))
    nb_x.wait_recv()
    o_norm[...] = nc[...] + nx[...]
    for k in offsets:
        rr_f[k].wait_recv()
    total = rr[0]
    for x in range(1, n_ep):
        total = total + rr[x]
    o_gr[...] = total
    o_rnorm[...] = jnp.sum(total * total, axis=0, keepdims=True)
    for k in offsets:
        ret_f[k].wait_recv()
    o_tok[...] = (contract(all_sel, home[...].reshape(n_exp * cap, fb), ((0,), (0,)))
                  + router_term).astype(BF16)
    for copy in started:
        copy.wait_send()


def flush(*refs):
    sem = refs[-1]
    copies = [pltpu.make_async_copy(refs[i], refs[9 + i], sem.at[i]) for i in range(9)]
    for copy in copies:
        copy.start()
    for copy in copies:
        copy.wait()


def fused(tokens, cotangent, routing, router_weight, gate_weight, up_weight, down_weight):
    n_ep, n_tp = lax.axis_size("ep"), lax.axis_size("tp")
    toks, width = tokens.shape
    n_exp = router_weight.shape[1]
    cap = max(2, 2 * toks * routing.shape[1] // n_exp)
    hid = gate_weight.shape[2]
    fb = width // n_tp
    two = 2 * cap
    slots = n_ep * cap
    span = width // n_ep
    copies = 16 * n_ep
    results = [
        ((toks, fb), BF16),
        ((routing.shape[1], toks), F32),
        ((n_exp, span), F32),
        ((width, hid), BF16),
        ((width, hid), BF16),
        ((hid, width), BF16),
        ((2, width), F32),
        ((1, hid), F32),
        ((1, span), F32),
    ]
    vmem = pl.BlockSpec(memory_space=pltpu.VMEM)
    hbm = pl.BlockSpec(memory_space=pltpu.HBM)
    outs = pl.pallas_call(
        functools.partial(kernel, n_ep, n_tp, cap),
        out_shape=[pltpu.VMEM(shape, dtype) for shape, dtype in results],
        in_specs=[hbm] * 7,
        out_specs=[vmem] * 9,
        scratch_shapes=[
            pltpu.VMEM((routing.shape[1], toks), jnp.int32),
            pltpu.VMEM((n_exp, width), BF16),
            pltpu.VMEM((toks, width), BF16),
            pltpu.VMEM((toks, width), BF16),
            pltpu.VMEM((width, 2 * hid), BF16),
            pltpu.VMEM((hid, width), BF16),
            pltpu.VMEM((n_exp, cap, toks), BF16),
            pltpu.VMEM((n_ep // 2, 2, toks, fb), BF16),
            pltpu.VMEM((n_ep // 2, n_exp, toks), F32),
            pltpu.VMEM((2, toks, fb), BF16),
            pltpu.VMEM((n_ep // 2, 2, cap, fb), BF16),
            pltpu.VMEM((2, cap, fb), BF16),
            pltpu.VMEM((n_tp, n_ep, 2, cap, fb), BF16),
            pltpu.VMEM((n_exp, 8, two), F32),
            pltpu.VMEM((n_ep, 8, two), F32),
            pltpu.VMEM((n_tp, n_ep, cap, fb), BF16),
            pltpu.VMEM((2, n_ep, cap, fb), BF16),
            pltpu.VMEM((n_ep, cap, fb), BF16),
            pltpu.VMEM((n_ep, cap, fb), BF16),
            pltpu.VMEM((n_ep, cap, fb), BF16),
            pltpu.VMEM((n_exp, cap, fb), BF16),
            pltpu.VMEM((slots, 2 * hid), BF16),
            pltpu.VMEM((slots, hid), BF16),
            pltpu.VMEM((n_ep // 2, 8, two), F32),
            pltpu.VMEM((n_ep // 2, 8, two), F32),
            pltpu.VMEM((n_ep // 2, 8, two), F32),
            pltpu.VMEM((n_exp, 8, two), F32),
            pltpu.VMEM((2, width), F32),
            pltpu.VMEM((2, width), F32),
            pltpu.VMEM((2, width), F32),
            pltpu.VMEM((n_exp, width), F32),
            pltpu.VMEM((n_ep, n_exp, span), F32),
            pltpu.SemaphoreType.DMA((11,)),
            pltpu.SemaphoreType.DMA((copies,)),
            pltpu.SemaphoreType.DMA((copies,)),
        ],
        compiler_params=pltpu.CompilerParams(
            collective_id=0, has_side_effects=True, vmem_limit_bytes=40 << 20
        ),
    )(*[pltpu.with_memory_space_constraint(v, pltpu.HBM)
        for v in (tokens, cotangent, routing.T, router_weight.T,
                  gate_weight[0], up_weight[0], down_weight[0])])
    outs = pl.pallas_call(
        flush,
        out_shape=[jax.ShapeDtypeStruct(shape, dtype) for shape, dtype in results],
        in_specs=[vmem] * 9,
        out_specs=[hbm] * 9,
        scratch_shapes=[pltpu.SemaphoreType.DMA((9,))],
    )(*[pltpu.with_memory_space_constraint(v, pltpu.VMEM) for v in outs])
    o_tok, o_gg, o_gr, o_gate, o_up, o_down, o_norm, o_dnorm, o_rnorm = outs
    return (o_tok, o_gg.T, o_gr.T, o_gate[None], o_up[None], o_down[None], o_norm[None],
            o_dnorm, o_rnorm[0])


def shards(tokens, cotangent, routing, router_weight, gate_weight, up_weight, down_weight):
    n_ep, n_tp = lax.axis_size("ep"), lax.axis_size("tp")
    toks, width = tokens.shape
    n_exp = router_weight.shape[1]
    cap = max(2, 2 * toks * routing.shape[1] // n_exp)
    fits = (
        n_tp == 4 and n_ep == 8 and n_ep == n_exp
        and 2 * cap == toks == 128 and gate_weight.shape[2] == 128
        and routing.shape[1] == 2 and width % (128 * 8) == 0
    )
    form = fused if fits else general
    return form(tokens, cotangent, routing, router_weight, gate_weight, up_weight, down_weight)


def solution(mesh):
    in_specs = (
        P("ep", None),
        P("ep", None),
        P("ep", None),
        P(),
        P("ep", None, "tp"),
        P("ep", None, "tp"),
        P("ep", "tp", None),
    )
    out_specs = (
        P("ep", "tp"),
        P("ep", None),
        P("ep", None),
        P("ep", None, "tp"),
        P("ep", None, "tp"),
        P("ep", "tp", None),
        P("ep", None, None),
        P("ep", "tp"),
        P("ep"),
    )
    return jax.shard_map(shards, mesh=mesh, in_specs=in_specs, out_specs=out_specs, check_vma=False)
```

```python
import functools
import math

import jax
import jax.numpy as jnp
from jax import lax
from jax.experimental import pallas as pl
from jax.experimental.pallas import tpu as pltpu
from jax.sharding import PartitionSpec as P


def silu_parts(pre_gate):
    sigmoid_gate = jax.nn.sigmoid(pre_gate)
    return (pre_gate * sigmoid_gate, sigmoid_gate * (1.0 + pre_gate * (1.0 - sigmoid_gate)))


def slot_layout(routing, experts_all, capacity):
    tok_count, top_count = routing.shape
    flat_expert = routing.reshape(-1)
    one_hot = (flat_expert[:, None] == jnp.arange(experts_all, dtype=jnp.int32)[None, :]).astype(
        jnp.int32
    )
    earlier = jnp.cumsum(one_hot, axis=0) - one_hot
    within = jnp.sum(earlier * one_hot, axis=1)
    position = flat_expert * capacity + within
    vacant = jnp.full((experts_all * capacity,), tok_count * top_count, jnp.int32)
    return (vacant.at[position].set(jnp.arange(tok_count * top_count, dtype=jnp.int32)), position)


def general(tokens, cotangent, routing, router_weight, gate_weight, up_weight, down_weight):
    tok_count, model_width = tokens.shape
    top_count = routing.shape[1]
    experts_all = router_weight.shape[1]
    expert_local = gate_weight.shape[0]
    ep_size = lax.axis_size("ep")
    tp_size = lax.axis_size("tp")
    tp_index = lax.axis_index("tp")
    slice_width = model_width // tp_size
    capacity = max(2, 2 * tok_count * top_count // experts_all)
    arrived = ep_size * capacity
    logits = jnp.dot(tokens, router_weight, preferred_element_type=jnp.float32)
    picked = (
        routing[:, :, None] == jnp.arange(experts_all, dtype=jnp.int32)[None, None, :]
    ).astype(jnp.float32)
    scores = jax.nn.sigmoid(jnp.einsum("tke,te->tk", picked, logits))
    score_sum = jnp.sum(scores, axis=1, keepdims=True)
    gating = scores / score_sum
    assignment, position = slot_layout(routing, experts_all, capacity)
    source_row = assignment // top_count
    padded_tokens = jnp.concatenate([tokens, jnp.zeros((1, model_width), tokens.dtype)], axis=0)
    padded_cotangent = jnp.concatenate(
        [cotangent, jnp.zeros((1, model_width), cotangent.dtype)], axis=0
    )
    padded_gating = jnp.concatenate([gating.reshape(-1), jnp.zeros((1,), jnp.float32)])
    sent_gating = padded_gating[assignment].reshape(experts_all, capacity)
    own_tokens = lax.dynamic_slice_in_dim(padded_tokens, tp_index * slice_width, slice_width, 1)
    own_cotangent = lax.dynamic_slice_in_dim(
        padded_cotangent, tp_index * slice_width, slice_width, 1
    )
    part_tokens, part_cotangent = (
        lax.all_to_all(
            own_tokens[source_row].reshape(experts_all, capacity, slice_width),
            "ep",
            split_axis=0,
            concat_axis=0,
            tiled=True,
        ),
        lax.all_to_all(
            own_cotangent[source_row].reshape(experts_all, capacity, slice_width),
            "ep",
            split_axis=0,
            concat_axis=0,
            tiled=True,
        ),
    )
    got_tokens, got_cotangent = (
        lax.all_gather(part_tokens, "tp", axis=2, tiled=True),
        lax.all_gather(part_cotangent, "tp", axis=2, tiled=True),
    )
    got_gating = lax.all_to_all(sent_gating, "ep", split_axis=0, concat_axis=0, tiled=True)

    def by_expert(values):
        shaped = values.reshape((ep_size, expert_local) + values.shape[1:])
        return jnp.moveaxis(shaped, 1, 0).reshape((expert_local, arrived) + values.shape[2:])

    def by_source(values):
        shaped = values.reshape((expert_local, ep_size, capacity) + values.shape[2:])
        return jnp.moveaxis(shaped, 1, 0).reshape(
            (ep_size * expert_local, capacity) + values.shape[2:]
        )

    rows_in = by_expert(got_tokens)
    cot_rows = by_expert(got_cotangent)
    slot_gating = by_expert(got_gating)[:, :, None]
    pre_gate = jnp.einsum("lrd,ldf->lrf", rows_in, gate_weight, preferred_element_type=jnp.float32)
    pre_up = jnp.einsum("lrd,ldf->lrf", rows_in, up_weight, preferred_element_type=jnp.float32)
    activated, silu_slope = silu_parts(pre_gate)
    hidden = (activated * pre_up).astype(jnp.bfloat16)
    back_raw = jnp.einsum("lrd,lfd->lrf", cot_rows, down_weight, preferred_element_type=jnp.float32)
    hidden_wide = hidden.astype(jnp.float32)
    gate_partial = jnp.sum(hidden_wide * back_raw, axis=2)
    scaled_back = slot_gating * back_raw
    grad_pre_gate = (scaled_back * pre_up * silu_slope).astype(jnp.bfloat16)
    grad_pre_up = (scaled_back * activated).astype(jnp.bfloat16)
    scaled_hidden = (slot_gating * hidden_wide).astype(jnp.bfloat16)
    gate_sum = jnp.einsum(
        "lrd,lrf->ldf", rows_in, grad_pre_gate, preferred_element_type=jnp.float32
    )
    up_sum = jnp.einsum("lrd,lrf->ldf", rows_in, grad_pre_up, preferred_element_type=jnp.float32)
    down_sum = jnp.einsum(
        "lrf,lrd->lfd", scaled_hidden, cot_rows, preferred_element_type=jnp.float32
    )
    down_norms = jnp.sum(down_sum * down_sum, axis=2)
    back_partial = jnp.einsum(
        "lrf,ldf->lrd", grad_pre_gate, gate_weight, preferred_element_type=jnp.float32
    ) + jnp.einsum("lrf,ldf->lrd", grad_pre_up, up_weight, preferred_element_type=jnp.float32)
    back_rounded = back_partial.astype(jnp.bfloat16)
    slot_values = (
        lax.psum_scatter(back_rounded, "tp", scatter_dimension=2, tiled=True)
        .astype(jnp.float32)
        .astype(jnp.bfloat16)
    )
    gating_total, gate_rows, up_rows = lax.psum(
        (gate_partial, jnp.sum(gate_sum * gate_sum, axis=2), jnp.sum(up_sum * up_sum, axis=2)), "tp"
    )
    home_values = lax.all_to_all(
        by_source(slot_values), "ep", split_axis=0, concat_axis=0, tiled=True
    )
    home_gating = lax.all_to_all(
        by_source(gating_total), "ep", split_axis=0, concat_axis=0, tiled=True
    )
    flat_values = home_values.reshape(experts_all * capacity, slice_width)
    token_terms = (
        flat_values[position].reshape(tok_count, top_count, slice_width).astype(jnp.float32)
    )
    grad_gating = home_gating.reshape(-1)[position].reshape(tok_count, top_count)
    weighted = jnp.sum(gating * grad_gating, axis=1, keepdims=True)
    grad_scores = (grad_gating - weighted) / score_sum
    grad_chosen = grad_scores * scores * (1.0 - scores)
    grad_logits = jnp.einsum("tk,tke->te", grad_chosen, picked).astype(jnp.bfloat16)
    router_slice = lax.dynamic_slice_in_dim(router_weight, tp_index * slice_width, slice_width, 0)
    router_term = jnp.einsum(
        "te,de->td", grad_logits, router_slice, preferred_element_type=jnp.float32
    )
    grad_tokens = (jnp.sum(token_terms, axis=1) + router_term).astype(jnp.bfloat16)
    grad_router = lax.psum_scatter(
        jnp.einsum("td,te->de", tokens, grad_logits, preferred_element_type=jnp.float32),
        "ep",
        scatter_dimension=0,
        tiled=True,
    )
    router_norms = jnp.sum(grad_router * grad_router, axis=1)
    in_norms = jnp.stack([gate_rows, up_rows], axis=1)
    return (
        grad_tokens,
        grad_gating,
        grad_router,
        gate_sum.astype(jnp.bfloat16),
        up_sum.astype(jnp.bfloat16),
        down_sum.astype(jnp.bfloat16),
        in_norms,
        down_norms,
        router_norms,
    )


MESH = pl.DeviceIdType.MESH
RAW, TO_Y, TO_X, TO_CORE, BACK, HOME, SMALL = range(7)
F32 = jnp.float32
BF16 = jnp.bfloat16


def contract(a, b, dims, precision=None):
    return lax.dot_general(
        a, b, ((dims[0], dims[1]), ((), ())), precision=precision, preferred_element_type=F32
    )


def flipped(index, mask, bits):
    out = index
    for bit in range(bits):
        if (mask >> bit) & 1:
            out = out + (1 << bit) * (1 - 2 * ((index // (1 << bit)) % 2))
    return out


def kernel(n_ep, n_tp, cap,
           tok_hbm, cot_hbm, rt_hbm, rw_hbm, wg, wu, wd_hbm,
           o_tok, o_gg, o_gr, o_gate, o_up, o_down, o_norm, o_dnorm, o_rnorm,
           rt, rw, tok, cot, wgu, wd, sel, raw, info, other_x, raw_x, ysa, ysx, ysw, arr_a, gall, mid, part, pc, xs, xr,
           fin, home, gp, sh, ggb, ggc, ggs, ggh, gts, nb, nc, nx, rp, rr, lsem, ssem, rsem):
    e = lax.axis_index("ep")
    p = lax.axis_index("tp")
    z, y = e // 2, e % 2
    x_me = p // 2
    toks, width = tok.shape
    n_exp = rw.shape[0]
    fb = width // n_tp
    hid = wd.shape[0]
    two = 2 * cap
    p_core, p_x, p_both = (flipped(p, m, 2) for m in (1, 2, 3))
    z_pair, z_mid = flipped(z, 1, 1), 3 - z
    is_mid = (z == 1) | (z == 2)
    is_edge = jnp.logical_not(is_mid)
    planes = (z, z_pair, 2 - z // 2, 3 - 3 * (z // 2))
    e_y = z * 2 + 1 - y
    sends, slots, local, branch = {}, {}, [], ["all"]

    def ep_of(plane, h=0):
        return plane * 2 + (y + h) % 2

    def receiver(arrival):
        return slots.setdefault(arrival, len(slots))

    def transfer(group, arrival, source, dest, ep=None, tp=None):
        return pltpu.make_async_remote_copy(
            src_ref=source, dst_ref=dest, send_sem=ssem.at[group],
            recv_sem=rsem.at[receiver(arrival)],
            device_id=(e if ep is None else ep, p if tp is None else tp), device_id_type=MESH)

    def send(key, source, dest, group, ep=None, tp=None, arrival=None):
        transfer(group, key if arrival is None else arrival, source, dest, ep, tp).start()
        unit = n_exp * 128 if group == SMALL else cap * fb
        sends[branch[-1], key] = (group, math.prod(source.shape) // unit)

    def only(cond, name, body):
        @pl.when(cond)
        def _():
            branch.append(name)
            body()
            branch.pop()

    def landed(arrival, ref):
        transfer(0, arrival, ref, ref).wait_recv()

    def load(source, dest):
        copy = pltpu.make_async_copy(source, dest, lsem.at[len(local)])
        copy.start()
        local.append(copy)
        return copy

    barrier = pltpu.get_barrier_semaphore()
    pl.semaphore_signal(barrier, inc=1, device_id=(ep_of(z_pair), p), device_id_type=MESH)

    @pl.when(is_mid)
    def _():
        pl.semaphore_signal(barrier, inc=1, device_id=(ep_of(z_mid), p), device_id_type=MESH)

    for ep, tp in ((e_y, p_x), (e_y, p), (e, p_x), (e, p_core)):
        pl.semaphore_signal(barrier, inc=1, device_id=(ep, tp), device_id_type=MESH)
    routing_in = load(rt_hbm, rt)
    cols = pl.ds(pl.multiple_of(p * fb, 128), fb)
    cols_x = pl.ds(pl.multiple_of(p_x * fb, 128), fb)
    raw_in = [load(tok_hbm.at[:, cols], raw.at[z, 0]), load(cot_hbm.at[:, cols], raw.at[z, 1])]
    raw_in += [load(tok_hbm.at[:, cols_x], other_x.at[0]), load(cot_hbm.at[:, cols_x], other_x.at[1])]
    full_in = [load(rw_hbm, rw), load(tok_hbm, tok), load(cot_hbm, cot)]
    weights_in = [load(wg, wgu.at[:, pl.ds(0, hid)]), load(wu, wgu.at[:, pl.ds(hid, hid)]),
                  load(wd_hbm, wd)]

    routing_in.wait()
    r0, r1 = rt[0:1, :], rt[1:2, :]
    row_e = lax.broadcasted_iota(jnp.int32, (128, toks), 0)
    member_t = (r0 == row_e) | (r1 == row_e)
    earlier = (lax.broadcasted_iota(jnp.int32, (toks, toks), 0)
               < lax.broadcasted_iota(jnp.int32, (toks, toks), 1))
    place_t = contract(member_t.astype(F32).astype(BF16), earlier.astype(F32).astype(BF16),
                       ((1,), (0,)))
    place_t = jnp.where(member_t, place_t, -1000.0)[:n_exp]
    member_t = member_t[:n_exp]
    info[z] = place_t
    slot_id = lax.broadcasted_iota(jnp.int32, (cap, toks), 0).astype(F32)

    for copy in raw_in:
        copy.wait()
    pl.semaphore_wait(barrier, 5 + is_mid.astype(jnp.int32))

    def group_of(kind):
        return RAW if kind[0] == "raw" else SMALL

    def along(kind, ref, s):
        if s == 0:
            send((kind, "pair"), ref, ref, group_of(kind), ep=ep_of(z_pair), arrival=(kind, 1))

            only(is_mid, "mid", lambda: send((kind, "mid"), ref, ref, group_of(kind),
                                             ep=ep_of(z_mid), arrival=(kind, 2)))
        elif s == 1:
            send((kind, "mid1"), ref, ref, group_of(kind), ep=ep_of(z_mid), arrival=(kind, 3))
        else:
            send((kind, "out", s), ref, ref, group_of(kind), ep=ep_of(z_pair), arrival=(kind, s))

    along("info", info.at[z], 0)
    along(("raw", 0), raw.at[z, 0], 0)
    along(("raw", 1), raw.at[z, 1], 0)

    def wide():
        for a in (0, 1):
            send(("wide", a), other_x.at[a], raw_x.at[a], RAW, ep=ep_of(z_pair))


    def parts_of(s, a):
        plane = planes[s]
        own = [(("raw", a), raw.at[plane, a])]
        if a == 0:
            return [("info", info.at[plane])] + own
        return own + [("gall", gall.at[ep_of(plane)])]

    def pass_on(s, a):
        for kind, ref in parts_of(s, a):
            landed((kind, s), ref)
            along(kind, ref, s)

    def settle(s, a):
        for kind, ref in parts_of(s, a):
            landed((kind, s), ref)

    def chosen(s, x):
        return (info[planes[s], pl.ds(x, 1), :] == slot_id).astype(F32).astype(BF16)

    def core(key, a, block, src):
        ref = arr_a.at[block, src, a]
        send((key, a), ref, ref, TO_CORE, tp=p_core, arrival=("c", key[1], a))

    def pick(s, a, diagonal=1):
        plane = planes[s]
        src = ep_of(plane)
        if s:
            picks = jnp.concatenate([chosen(s, e_y), chosen(s, e)], axis=0)
        else:
            picks = chosen(s, e_y)
        rows = contract(picks, raw[plane, a], ((1,), (0,))).astype(BF16)
        ysa[plane, a] = rows[:cap]
        there = arr_a.at[p, src, a]
        send(("y", s, a), ysa.at[plane, a], there, TO_Y, ep=e_y)
        if s:
            if diagonal:
                send(("x", s, 1, a), ysa.at[plane, a], there, TO_X, ep=e_y, tp=p_x)
            arr_a[p, src, a] = rows[cap:]
            send(("x", s, 0, a), there, there, TO_X, tp=p_x)
            core(("c", s, 0), a, p, src)
            if a == 1:
                send(("gy", s), gall.at[src], gall.at[src], SMALL, ep=e_y)
        else:
            ysx[a] = contract(picks, other_x[a], ((1,), (0,))).astype(BF16)
            send(("yx", a), ysx.at[a], arr_a.at[p_x, src, a], TO_Y, ep=e_y, arrival=("y", 0, a))

    def pick_wide(a):
        src = ep_of(z_pair)
        picks = jnp.concatenate([chosen(1, e_y), chosen(1, e)], axis=0)
        for i, (block, source) in enumerate(((p, raw.at[z_pair, a]), (p_x, raw_x.at[a]))):
            if i:
                landed(("wide", a), raw_x.at[a])
            rows = contract(picks, source[...], ((1,), (0,))).astype(BF16)
            buffer = ysw.at[a] if i else ysa.at[z_pair, a]
            buffer[...] = rows[:cap]
            send(("yw", a, i), buffer, arr_a.at[block, src, a], TO_Y, ep=e_y, arrival=("yw", a))
            arr_a[block, src, a] = rows[cap:]
            core(("cw"[i], 1, 0), a, block, src)
        if a == 1:
            send(("gy", 1), gall.at[src], gall.at[src], SMALL, ep=e_y)

    def from_y_wide(a):
        src = ep_of(z_pair, 1)
        landed(("yw", a), ysx)
        core(("c", 1, 1), a, p, src)
        core(("c2", 1, 1), a, p_x, src)

    def from_y(s, a, diagonal=1):
        src = ep_of(planes[s], 1)
        landed(("y", s, a), arr_a.at[p, src, a] if s else ysx)
        if not diagonal:
            send(("x", s, 1, a), arr_a.at[p, src, a], arr_a.at[p, src, a], TO_X, tp=p_x)
        core(("c", s, 1), a, p, src)
        if s == 0:
            core(("c2", s, 1), a, p_x, src)

    def from_x(s, h, a):
        src = ep_of(planes[s], h)
        landed(("x", s, h, a), arr_a.at[p_x, src, a])
        core(("c2", s, h), a, p_x, src)

    def gathered(s, a):
        landed(("c", s, a), arr_a.at[0, pl.ds(0, 2)] if s else ysx)

    def compute_a(s):
        gathered(s, 0)
        pair = pl.ds(planes[s] * 2, 2)
        pre = jnp.zeros((two, 2 * hid), F32)
        for b in range(n_tp):
            c = slice(b * fb, (b + 1) * fb)
            pre = pre + contract(arr_a[b, pair, 0].reshape(two, fb), wgu[c, :], ((1,), (0,)))
        pre_gate, pre_up = pre[:, :hid], pre[:, hid:]
        activated, slope = silu_parts(pre_gate)
        mid[s, 0] = activated
        mid[s, 1] = pre_up * slope
        mid[s, 2] = (activated * pre_up).astype(BF16).astype(F32)

    def compute_b(s):
        plane = planes[s]
        base = plane * 2
        gathered(s, 1)
        landed(("gy", s), gall.at[ep_of(plane, 1)])
        pair = pl.ds(base, 2)
        here = pl.ds(pl.multiple_of(base * cap, two), two)
        back = jnp.zeros((two, hid), F32)
        for b in range(n_tp):
            c = slice(b * fb, (b + 1) * fb)
            back = back + contract(arr_a[b, pair, 1].reshape(two, fb), wd[:, c], ((1,), (1,)))
        gate = jnp.concatenate([jnp.sum(jnp.where(
            gall[base + i, pl.ds(n_exp + e, 1), :] == slot_id, gall[base + i, pl.ds(e, 1), :], 0.0),
            axis=1, keepdims=True) for i in (0, 1)], axis=0)
        hidden = mid[s, 2]
        scaled = gate * back
        grads = jnp.concatenate([(scaled * mid[s, 1]).astype(BF16),
                                 (scaled * mid[s, 0]).astype(BF16)], axis=1)
        for i, b in ((1, p_both), (0, p_core)):
            wb = wgu[pl.ds(pl.multiple_of(b * fb, 128), fb), :]
            part[b, pair] = contract(grads, wb, ((1,), (1,))).astype(BF16).reshape(2, cap, fb)
            send(("pc", s, i), part.at[b, pair], pc.at[i, pair], BACK, tp=p_core)
        ggb[plane] = contract(jnp.ones((8, hid), F32), hidden * back, ((1,), (1,)),
                              lax.Precision.HIGHEST)
        send(("ggc", s), ggb.at[plane], ggc.at[plane], SMALL, tp=p_core)
        for b in (p_x, p):
            wb = wgu[pl.ds(pl.multiple_of(b * fb, 128), fb), :]
            part[b, pair] = contract(grads, wb, ((1,), (1,))).astype(BF16).reshape(2, cap, fb)
        gp[here, :] = grads
        sh[here, :] = (gate * hidden).astype(BF16)

    def gate_home(s):
        plane = planes[s]
        landed(("ggc", s), ggc.at[plane])
        ggs[plane] = ggb[plane] + ggc[plane]
        for h in (0, 1):
            for far, tp in ((0, p), (1, p_x)):
                if s == 0 and h == 0 and far == 0:
                    ggh[e, x_me] = ggs[plane]
                else:
                    send(("ggh", s, h, far), ggs.at[plane], ggh.at[e, x_me], SMALL,
                         ep=ep_of(plane, h), tp=tp, arrival="ggh" if s or h else "ggh2")

    def to_x(s):
        pair = pl.ds(planes[s] * 2, 2)
        landed(("pc", s, 1), pc.at[1, pair])
        xs[pair] = (part[p_x, pair].astype(F32) + pc[1, pair].astype(F32)).astype(BF16)
        for h in (0, 1):
            src = ep_of(planes[s], h)
            send(("xs", s, h), xs.at[src], xr.at[src], BACK, tp=p_x)
        landed(("pc", s, 0), pc.at[0, pair])

    def to_home(s, h):
        other = ep_of(planes[s], h)
        landed(("xs", s, h), xr.at[other])
        fin[other] = (part[p, other].astype(F32) + pc[0, other].astype(F32)
                      + xr[other].astype(F32)).astype(BF16)
        if s or h:
            send(("fin", s, h), fin.at[other], home.at[e], HOME, ep=other, arrival="fin")
        else:
            home[e] = fin[e]

    def in_block(b):
        rows = arr_a[b, :, 0].reshape(n_ep * cap, fb)
        sums = contract(gp[...], rows, ((0,), (0,)))
        c = slice(b * fb, (b + 1) * fb)
        o_gate[c, :] = jnp.transpose(sums[:hid]).astype(BF16)
        o_up[c, :] = jnp.transpose(sums[hid:]).astype(BF16)
        nb[0:1, c] = jnp.sum(sums[:hid] * sums[:hid], axis=0, keepdims=True)
        nb[1:2, c] = jnp.sum(sums[hid:] * sums[hid:], axis=0, keepdims=True)

    def down():
        dn = jnp.zeros((hid, 1), F32)
        for b in range(n_tp):
            sums = contract(sh[...], arr_a[b, :, 1].reshape(n_ep * cap, fb), ((0,), (0,)))
            o_down[:, b * fb:(b + 1) * fb] = sums.astype(BF16)
            dn = dn + jnp.sum(sums * sums, axis=1, keepdims=True)
        o_dnorm[...] = jnp.transpose(jnp.broadcast_to(dn, (hid, 128)))[0:1, :]

    pick(0, 0)
    pick(0, 1)

    for copy in full_in[:2]:
        copy.wait()
    logits_t = contract(rw[...], tok[...], ((1,), (1,)))
    score_t = jnp.where(member_t, jax.nn.sigmoid(logits_t), 0.0)
    score_sum = jnp.sum(score_t, axis=0, keepdims=True)
    gating_t = score_t / score_sum
    gall[e, 0:n_exp] = gating_t
    gall[e, n_exp:2 * n_exp] = place_t
    along("gall", gall.at[e], 0)
    only(is_edge, "edge", wide)
    send(("gy", 0), gall.at[e], gall.at[e], SMALL, ep=e_y)
    for x in range(n_exp):
        sel[x] = (place_t[x:x + 1, :] == slot_id).astype(F32).astype(BF16)
    full_in[2].wait()
    for a, ref in enumerate((tok, cot)):
        rows = contract(sel[e], ref[...], ((1,), (0,))).astype(BF16)
        for b in range(n_tp):
            arr_a[b, e, a] = rows[:, b * fb:(b + 1) * fb]
    for copy in weights_in:
        copy.wait()

    def mid_plane():
        pass_on(1, 0)
        pass_on(2, 0)
        pick(2, 0)
        pass_on(1, 1)
        pass_on(2, 1)
        pick(2, 1)
        from_y(0, 0)
        from_y(0, 1)
        compute_a(0)
        pass_on(3, 0)
        pick(3, 0)
        compute_b(0)
        from_x(2, 0, 0)
        from_y(2, 0)
        from_x(2, 1, 0)
        gate_home(0)
        pass_on(3, 1)
        pick(3, 1)
        pick_wide(0)
        pick_wide(1)
        from_x(2, 0, 1)
        from_y(2, 1)
        from_x(2, 1, 1)
        compute_a(2)
        compute_b(2)
        from_x(3, 0, 0)
        from_y(3, 0)
        from_x(3, 1, 0)
        gate_home(2)
        to_x(2)
        to_x(0)
        compute_a(3)
        from_x(3, 0, 1)
        from_y(3, 1)
        from_x(3, 1, 1)
        compute_b(3)
        to_home(2, 0)
        from_y_wide(0)
        to_home(2, 1)
        gate_home(3)
        to_x(3)
        compute_a(1)
        from_y_wide(1)
        compute_b(1)
        to_home(3, 0)
        in_block(0)
        in_block(1)
        to_home(3, 1)
        gate_home(1)
        to_x(1)
        in_block(2)
        in_block(3)
        send("nbc", nb, nc, SMALL, tp=p_core)
        down()
        landed("nbc", nc)
        nc[...] = nb[...] + nc[...]
        send("nbx", nc, nx, SMALL, tp=p_x)
        to_home(1, 0)
        to_home(1, 1)

    def edge_plane():
        settle(1, 0)
        pick(1, 0, 0)
        settle(1, 1)
        pick(1, 1, 0)
        from_y(1, 0, 0)
        settle(2, 0)
        pick(2, 0)
        from_y(1, 1, 0)
        from_y(0, 0)
        from_y(0, 1)
        compute_a(0)
        settle(2, 1)
        pick(2, 1)
        compute_b(0)
        from_x(1, 0, 0)
        from_x(1, 1, 0)
        gate_home(0)
        from_x(1, 0, 1)
        compute_a(1)
        settle(3, 0)
        pick(3, 0)
        from_x(1, 1, 1)
        from_x(2, 0, 0)
        from_y(2, 0)
        compute_b(1)
        settle(3, 1)
        pick(3, 1)
        from_x(2, 1, 0)
        gate_home(1)
        to_x(1)
        compute_a(2)
        from_x(2, 0, 1)
        from_y(2, 1)
        from_x(2, 1, 1)
        compute_b(2)
        from_x(3, 0, 0)
        from_y(3, 0)
        from_x(3, 1, 0)
        gate_home(2)
        to_x(2)
        compute_a(3)
        from_x(3, 0, 1)
        from_y(3, 1)
        from_x(3, 1, 1)
        to_home(1, 0)
        compute_b(3)
        to_home(1, 1)
        in_block(0)
        gate_home(3)
        to_x(3)
        to_x(0)
        to_home(2, 0)
        in_block(1)
        to_home(2, 1)
        in_block(2)
        in_block(3)
        send("nbc", nb, nc, SMALL, tp=p_core)
        down()
        to_home(3, 0)
        landed("nbc", nc)
        nc[...] = nb[...] + nc[...]
        send("nbx", nc, nx, SMALL, tp=p_x)
        to_home(3, 1)

    only(is_mid, "mid", mid_plane)
    only(is_edge, "edge", edge_plane)


    landed("ggh", ggh.at[pl.ds(0, n_exp - 1)])
    landed("ggh2", ggh.at[0, 0])
    gts[0:n_exp, :] = ggh[:, 0, 0, :] + ggh[:, 1, 0, :]
    gts[...] = jnp.transpose(gts[...])
    mine = gts[pl.ds(pl.multiple_of(y * cap, 8), cap), :]
    got_t = jnp.concatenate([jnp.sum(jnp.where(
        place_t[x:x + 1, :] == slot_id, mine[:, x:x + 1], 0.0), axis=0, keepdims=True)
        for x in range(n_exp)], axis=0)
    for k, r in enumerate((r0, r1)):
        o_gg[k:k + 1, :] = jnp.sum(jnp.where(r == row_e[:n_exp], got_t, 0.0), axis=0, keepdims=True)
    weighted = jnp.sum(gating_t * got_t, axis=0, keepdims=True)
    grad_logits = jnp.where(member_t, (got_t - weighted) / score_sum * score_t * (1.0 - score_t),
                            0.0).astype(BF16)
    rp[...] = contract(grad_logits, tok[...], ((1,), (0,)))
    span = width // n_ep
    for s in (3, 2, 1, 0):
        for h in (0, 1):
            if s or h:
                other = ep_of(planes[s], h)
                send(("rr", s, h), rp.at[:, pl.ds(pl.multiple_of(other * span, 128), span)],
                     rr.at[e], SMALL, ep=other, arrival="rr")
    rr[e] = rp[:, pl.ds(pl.multiple_of(e * span, 128), span)]
    to_home(0, 1)
    to_home(0, 0)
    landed("nbx", nx)
    o_norm[...] = nc[...] + nx[...]
    landed("fin", home.at[pl.ds(0, n_ep - 1)])
    landed("rr", rr.at[pl.ds(0, n_ep - 1)])
    total = rr[0]
    for x in range(1, n_ep):
        total = total + rr[x]
    o_gr[...] = total
    o_rnorm[...] = jnp.sum(total * total, axis=0, keepdims=True)
    router_term = contract(grad_logits, rw[:, cols], ((0,), (0,)))
    all_sel = sel[...].reshape(n_exp * cap, toks)
    o_tok[...] = (contract(all_sel, home[...].reshape(n_exp * cap, fb), ((0,), (0,)))
                  + router_term).astype(BF16)
    def drain(name):
        for group in range(SMALL + 1):
            count = sum(n for (where, _), (g, n) in sends.items()
                        if g == group and where in ("all", name))
            if group == SMALL:
                d = next(d for d in (4, 2, 1) if count % d == 0)
                whole = mid.at[pl.ds(0, d), 0, pl.ds(0, count // d * n_exp)]
            else:
                d, k, j = next((d, k, j) for d in range(1, n_tp + 1) for j in (1, 2)
                               for k in range(1, n_ep + 1) if d * k * j == count)
                whole = arr_a.at[pl.ds(0, d), pl.ds(0, k), pl.ds(0, j)]
            transfer(group, "fin", whole, whole).wait_send()

    only(is_edge, "edge", lambda: drain("edge"))
    only(is_mid, "mid", lambda: drain("mid"))


def flush(*refs):
    sem = refs[-1]
    copies = [pltpu.make_async_copy(refs[i], refs[9 + i], sem.at[i]) for i in range(9)]
    for copy in copies:
        copy.start()
    for copy in copies:
        copy.wait()


def fused(tokens, cotangent, routing, router_weight, gate_weight, up_weight, down_weight):
    n_ep, n_tp = lax.axis_size("ep"), lax.axis_size("tp")
    toks, width = tokens.shape
    n_exp = router_weight.shape[1]
    cap = max(2, 2 * toks * routing.shape[1] // n_exp)
    hid = gate_weight.shape[2]
    fb = width // n_tp
    two = 2 * cap
    slots = n_ep * cap
    span = width // n_ep
    results = [
        ((toks, fb), BF16),
        ((routing.shape[1], toks), F32),
        ((n_exp, span), F32),
        ((width, hid), BF16),
        ((width, hid), BF16),
        ((hid, width), BF16),
        ((2, width), F32),
        ((1, hid), F32),
        ((1, span), F32),
    ]
    vmem = pl.BlockSpec(memory_space=pltpu.VMEM)
    hbm = pl.BlockSpec(memory_space=pltpu.HBM)
    outs = pl.pallas_call(
        functools.partial(kernel, n_ep, n_tp, cap),
        out_shape=[pltpu.VMEM(shape, dtype) for shape, dtype in results],
        in_specs=[hbm] * 7,
        out_specs=[vmem] * 9,
        scratch_shapes=[
            pltpu.VMEM((routing.shape[1], toks), jnp.int32),
            pltpu.VMEM((n_exp, width), BF16),
            pltpu.VMEM((toks, width), BF16),
            pltpu.VMEM((toks, width), BF16),
            pltpu.VMEM((width, 2 * hid), BF16),
            pltpu.VMEM((hid, width), BF16),
            pltpu.VMEM((n_exp, cap, toks), BF16),
            pltpu.VMEM((n_ep // 2, 2, toks, fb), BF16),
            pltpu.VMEM((n_ep // 2, n_exp, toks), F32),
            pltpu.VMEM((2, toks, fb), BF16),
            pltpu.VMEM((2, toks, fb), BF16),
            pltpu.VMEM((n_ep // 2, 2, cap, fb), BF16),
            pltpu.VMEM((2, cap, fb), BF16),
            pltpu.VMEM((2, cap, fb), BF16),
            pltpu.VMEM((n_tp, n_ep, 2, cap, fb), BF16),
            pltpu.VMEM((n_ep, 2 * n_exp, toks), F32),
            pltpu.VMEM((n_ep // 2, 3, two, hid), F32),
            pltpu.VMEM((n_tp, n_ep, cap, fb), BF16),
            pltpu.VMEM((2, n_ep, cap, fb), BF16),
            pltpu.VMEM((n_ep, cap, fb), BF16),
            pltpu.VMEM((n_ep, cap, fb), BF16),
            pltpu.VMEM((n_ep, cap, fb), BF16),
            pltpu.VMEM((n_exp, cap, fb), BF16),
            pltpu.VMEM((slots, 2 * hid), BF16),
            pltpu.VMEM((slots, hid), BF16),
            pltpu.VMEM((n_ep // 2, 8, two), F32),
            pltpu.VMEM((n_ep // 2, 8, two), F32),
            pltpu.VMEM((n_ep // 2, 8, two), F32),
            pltpu.VMEM((n_exp, 2, 8, two), F32),
            pltpu.VMEM((two, toks), F32),
            pltpu.VMEM((2, width), F32),
            pltpu.VMEM((2, width), F32),
            pltpu.VMEM((2, width), F32),
            pltpu.VMEM((n_exp, width), F32),
            pltpu.VMEM((n_ep, n_exp, span), F32),
            pltpu.SemaphoreType.DMA((11,)),
            pltpu.SemaphoreType.DMA((SMALL + 1,)),
            pltpu.SemaphoreType.DMA((80,)),
        ],
        compiler_params=pltpu.CompilerParams(
            collective_id=0, has_side_effects=True, vmem_limit_bytes=40 << 20
        ),
    )(*[pltpu.with_memory_space_constraint(v, pltpu.HBM)
        for v in (tokens, cotangent, routing.T, router_weight.T,
                  gate_weight[0], up_weight[0], down_weight[0])])
    outs = pl.pallas_call(
        flush,
        out_shape=[jax.ShapeDtypeStruct(shape, dtype) for shape, dtype in results],
        in_specs=[vmem] * 9,
        out_specs=[hbm] * 9,
        scratch_shapes=[pltpu.SemaphoreType.DMA((9,))],
    )(*[pltpu.with_memory_space_constraint(v, pltpu.VMEM) for v in outs])
    o_tok, o_gg, o_gr, o_gate, o_up, o_down, o_norm, o_dnorm, o_rnorm = outs
    return (o_tok, o_gg.T, o_gr.T, o_gate[None], o_up[None], o_down[None], o_norm[None],
            o_dnorm, o_rnorm[0])


def shards(tokens, cotangent, routing, router_weight, gate_weight, up_weight, down_weight):
    n_ep, n_tp = lax.axis_size("ep"), lax.axis_size("tp")
    toks, width = tokens.shape
    n_exp = router_weight.shape[1]
    cap = max(2, 2 * toks * routing.shape[1] // n_exp)
    fits = (
        n_tp == 4 and n_ep == 8 and n_ep == n_exp
        and 2 * cap == toks == 128 and gate_weight.shape[2] == 128
        and routing.shape[1] == 2 and width % (128 * 8) == 0
    )
    form = fused if fits else general
    return form(tokens, cotangent, routing, router_weight, gate_weight, up_weight, down_weight)


def solution(mesh):
    in_specs = (
        P("ep", None),
        P("ep", None),
        P("ep", None),
        P(),
        P("ep", None, "tp"),
        P("ep", None, "tp"),
        P("ep", "tp", None),
    )
    out_specs = (
        P("ep", "tp"),
        P("ep", None),
        P("ep", None),
        P("ep", None, "tp"),
        P("ep", None, "tp"),
        P("ep", "tp", None),
        P("ep", None, None),
        P("ep", "tp"),
        P("ep"),
    )
    return jax.shard_map(shards, mesh=mesh, in_specs=in_specs, out_specs=out_specs, check_vma=False)
```

```python
import functools
import math

import jax
import jax.numpy as jnp
from jax import lax
from jax.experimental import pallas as pl
from jax.experimental.pallas import tpu as pltpu
from jax.sharding import PartitionSpec as P


def silu_parts(pre_gate):
    sigmoid_gate = jax.nn.sigmoid(pre_gate)
    return (pre_gate * sigmoid_gate, sigmoid_gate * (1.0 + pre_gate * (1.0 - sigmoid_gate)))


def slot_layout(routing, experts_all, capacity):
    tok_count, top_count = routing.shape
    flat_expert = routing.reshape(-1)
    one_hot = (flat_expert[:, None] == jnp.arange(experts_all, dtype=jnp.int32)[None, :]).astype(
        jnp.int32
    )
    earlier = jnp.cumsum(one_hot, axis=0) - one_hot
    within = jnp.sum(earlier * one_hot, axis=1)
    position = flat_expert * capacity + within
    vacant = jnp.full((experts_all * capacity,), tok_count * top_count, jnp.int32)
    return (vacant.at[position].set(jnp.arange(tok_count * top_count, dtype=jnp.int32)), position)


def general(tokens, cotangent, routing, router_weight, gate_weight, up_weight, down_weight):
    tok_count, model_width = tokens.shape
    top_count = routing.shape[1]
    experts_all = router_weight.shape[1]
    expert_local = gate_weight.shape[0]
    ep_size = lax.axis_size("ep")
    tp_size = lax.axis_size("tp")
    tp_index = lax.axis_index("tp")
    slice_width = model_width // tp_size
    capacity = max(2, 2 * tok_count * top_count // experts_all)
    arrived = ep_size * capacity
    logits = jnp.dot(tokens, router_weight, preferred_element_type=jnp.float32)
    picked = (
        routing[:, :, None] == jnp.arange(experts_all, dtype=jnp.int32)[None, None, :]
    ).astype(jnp.float32)
    scores = jax.nn.sigmoid(jnp.einsum("tke,te->tk", picked, logits))
    score_sum = jnp.sum(scores, axis=1, keepdims=True)
    gating = scores / score_sum
    assignment, position = slot_layout(routing, experts_all, capacity)
    source_row = assignment // top_count
    padded_tokens = jnp.concatenate([tokens, jnp.zeros((1, model_width), tokens.dtype)], axis=0)
    padded_cotangent = jnp.concatenate(
        [cotangent, jnp.zeros((1, model_width), cotangent.dtype)], axis=0
    )
    padded_gating = jnp.concatenate([gating.reshape(-1), jnp.zeros((1,), jnp.float32)])
    sent_gating = padded_gating[assignment].reshape(experts_all, capacity)
    own_tokens = lax.dynamic_slice_in_dim(padded_tokens, tp_index * slice_width, slice_width, 1)
    own_cotangent = lax.dynamic_slice_in_dim(
        padded_cotangent, tp_index * slice_width, slice_width, 1
    )
    part_tokens, part_cotangent = (
        lax.all_to_all(
            own_tokens[source_row].reshape(experts_all, capacity, slice_width),
            "ep",
            split_axis=0,
            concat_axis=0,
            tiled=True,
        ),
        lax.all_to_all(
            own_cotangent[source_row].reshape(experts_all, capacity, slice_width),
            "ep",
            split_axis=0,
            concat_axis=0,
            tiled=True,
        ),
    )
    got_tokens, got_cotangent = (
        lax.all_gather(part_tokens, "tp", axis=2, tiled=True),
        lax.all_gather(part_cotangent, "tp", axis=2, tiled=True),
    )
    got_gating = lax.all_to_all(sent_gating, "ep", split_axis=0, concat_axis=0, tiled=True)

    def by_expert(values):
        shaped = values.reshape((ep_size, expert_local) + values.shape[1:])
        return jnp.moveaxis(shaped, 1, 0).reshape((expert_local, arrived) + values.shape[2:])

    def by_source(values):
        shaped = values.reshape((expert_local, ep_size, capacity) + values.shape[2:])
        return jnp.moveaxis(shaped, 1, 0).reshape(
            (ep_size * expert_local, capacity) + values.shape[2:]
        )

    rows_in = by_expert(got_tokens)
    cot_rows = by_expert(got_cotangent)
    slot_gating = by_expert(got_gating)[:, :, None]
    pre_gate = jnp.einsum("lrd,ldf->lrf", rows_in, gate_weight, preferred_element_type=jnp.float32)
    pre_up = jnp.einsum("lrd,ldf->lrf", rows_in, up_weight, preferred_element_type=jnp.float32)
    activated, silu_slope = silu_parts(pre_gate)
    hidden = (activated * pre_up).astype(jnp.bfloat16)
    back_raw = jnp.einsum("lrd,lfd->lrf", cot_rows, down_weight, preferred_element_type=jnp.float32)
    hidden_wide = hidden.astype(jnp.float32)
    gate_partial = jnp.sum(hidden_wide * back_raw, axis=2)
    scaled_back = slot_gating * back_raw
    grad_pre_gate = (scaled_back * pre_up * silu_slope).astype(jnp.bfloat16)
    grad_pre_up = (scaled_back * activated).astype(jnp.bfloat16)
    scaled_hidden = (slot_gating * hidden_wide).astype(jnp.bfloat16)
    gate_sum = jnp.einsum(
        "lrd,lrf->ldf", rows_in, grad_pre_gate, preferred_element_type=jnp.float32
    )
    up_sum = jnp.einsum("lrd,lrf->ldf", rows_in, grad_pre_up, preferred_element_type=jnp.float32)
    down_sum = jnp.einsum(
        "lrf,lrd->lfd", scaled_hidden, cot_rows, preferred_element_type=jnp.float32
    )
    down_norms = jnp.sum(down_sum * down_sum, axis=2)
    back_partial = jnp.einsum(
        "lrf,ldf->lrd", grad_pre_gate, gate_weight, preferred_element_type=jnp.float32
    ) + jnp.einsum("lrf,ldf->lrd", grad_pre_up, up_weight, preferred_element_type=jnp.float32)
    back_rounded = back_partial.astype(jnp.bfloat16)
    slot_values = (
        lax.psum_scatter(back_rounded, "tp", scatter_dimension=2, tiled=True)
        .astype(jnp.float32)
        .astype(jnp.bfloat16)
    )
    gating_total, gate_rows, up_rows = lax.psum(
        (gate_partial, jnp.sum(gate_sum * gate_sum, axis=2), jnp.sum(up_sum * up_sum, axis=2)), "tp"
    )
    home_values = lax.all_to_all(
        by_source(slot_values), "ep", split_axis=0, concat_axis=0, tiled=True
    )
    home_gating = lax.all_to_all(
        by_source(gating_total), "ep", split_axis=0, concat_axis=0, tiled=True
    )
    flat_values = home_values.reshape(experts_all * capacity, slice_width)
    token_terms = (
        flat_values[position].reshape(tok_count, top_count, slice_width).astype(jnp.float32)
    )
    grad_gating = home_gating.reshape(-1)[position].reshape(tok_count, top_count)
    weighted = jnp.sum(gating * grad_gating, axis=1, keepdims=True)
    grad_scores = (grad_gating - weighted) / score_sum
    grad_chosen = grad_scores * scores * (1.0 - scores)
    grad_logits = jnp.einsum("tk,tke->te", grad_chosen, picked).astype(jnp.bfloat16)
    router_slice = lax.dynamic_slice_in_dim(router_weight, tp_index * slice_width, slice_width, 0)
    router_term = jnp.einsum(
        "te,de->td", grad_logits, router_slice, preferred_element_type=jnp.float32
    )
    grad_tokens = (jnp.sum(token_terms, axis=1) + router_term).astype(jnp.bfloat16)
    grad_router = lax.psum_scatter(
        jnp.einsum("td,te->de", tokens, grad_logits, preferred_element_type=jnp.float32),
        "ep",
        scatter_dimension=0,
        tiled=True,
    )
    router_norms = jnp.sum(grad_router * grad_router, axis=1)
    in_norms = jnp.stack([gate_rows, up_rows], axis=1)
    return (
        grad_tokens,
        grad_gating,
        grad_router,
        gate_sum.astype(jnp.bfloat16),
        up_sum.astype(jnp.bfloat16),
        down_sum.astype(jnp.bfloat16),
        in_norms,
        down_norms,
        router_norms,
    )


MESH = pl.DeviceIdType.MESH
RAW, TO_Y, TO_X, TO_CORE, BACK, HOME, SMALL = range(7)
F32 = jnp.float32
BF16 = jnp.bfloat16


def contract(a, b, dims, precision=None):
    return lax.dot_general(
        a, b, ((dims[0], dims[1]), ((), ())), precision=precision, preferred_element_type=F32
    )


def flipped(index, mask, bits):
    out = index
    for bit in range(bits):
        if (mask >> bit) & 1:
            out = out + (1 << bit) * (1 - 2 * ((index // (1 << bit)) % 2))
    return out


def kernel(n_ep, n_tp, cap,
           tok_hbm, cot_hbm, rt_hbm, rw_hbm, wg, wu, wd_hbm,
           o_tok, o_gg, o_gr, o_gate, o_up, o_down, o_norm, o_dnorm, o_rnorm,
           rt, rw, tok, cot, wgu, wd, sel, raw, info, other_x, raw_x, ysa, ysx, ysw, arr_a, gall, mid, part, pc, xs, xr,
           fin, home, gp, sh, ggb, ggc, ggs, ggh, gts, nb, nc, nx, gl, rp, rr, lsem, ssem, rsem, ready):
    e = lax.axis_index("ep")
    p = lax.axis_index("tp")
    z, y = e // 2, e % 2
    x_me = p // 2
    toks, width = tok.shape
    n_exp = rw.shape[0]
    fb = width // n_tp
    hid = wd.shape[0]
    two = 2 * cap
    p_core, p_x, p_both = (flipped(p, m, 2) for m in (1, 2, 3))
    z_pair, z_mid = flipped(z, 1, 1), 3 - z
    is_mid = (z == 1) | (z == 2)
    is_edge = jnp.logical_not(is_mid)
    planes = (z, z_pair, 2 - z // 2, 3 - 3 * (z // 2))
    e_y = z * 2 + 1 - y
    sends, slots, local, branch = {}, {}, [], ["all"]

    def ep_of(plane, h=0):
        return plane * 2 + (y + h) % 2

    def receiver(arrival):
        return slots.setdefault(arrival, len(slots))

    def transfer(group, arrival, source, dest, ep=None, tp=None):
        return pltpu.make_async_remote_copy(
            src_ref=source, dst_ref=dest, send_sem=ssem.at[group],
            recv_sem=rsem.at[receiver(arrival)],
            device_id=(e if ep is None else ep, p if tp is None else tp), device_id_type=MESH)

    def send(key, source, dest, group, ep=None, tp=None, arrival=None):
        transfer(group, key if arrival is None else arrival, source, dest, ep, tp).start()
        unit = n_exp * 128 if group == SMALL else cap * fb
        sends[branch[-1], key] = (group, math.prod(source.shape) // unit)

    def only(cond, name, body):
        @pl.when(cond)
        def _():
            branch.append(name)
            body()
            branch.pop()

    def landed(arrival, ref):
        transfer(0, arrival, ref, ref).wait_recv()

    def load(source, dest):
        copy = pltpu.make_async_copy(source, dest, lsem.at[len(local)])
        copy.start()
        local.append(copy)
        return copy

    barrier = pltpu.get_barrier_semaphore()
    pl.semaphore_signal(barrier, inc=1, device_id=(ep_of(z_pair), p), device_id_type=MESH)

    @pl.when(is_mid)
    def _():
        pl.semaphore_signal(barrier, inc=1, device_id=(ep_of(z_mid), p), device_id_type=MESH)

    for ep, tp in ((e_y, p), (e, p_x), (e, p_core)):
        pl.semaphore_signal(barrier, inc=1, device_id=(ep, tp), device_id_type=MESH)
    routing_in = load(rt_hbm, rt)
    cols = pl.ds(pl.multiple_of(p * fb, 128), fb)
    cols_x = pl.ds(pl.multiple_of(p_x * fb, 128), fb)
    raw_in = [load(tok_hbm.at[:, cols], raw.at[z, 0]), load(cot_hbm.at[:, cols], raw.at[z, 1])]
    raw_in += [load(tok_hbm.at[:, cols_x], other_x.at[0]), load(cot_hbm.at[:, cols_x], other_x.at[1])]
    full_in = [load(rw_hbm, rw), load(tok_hbm, tok), load(cot_hbm, cot)]
    weights_in = [load(wg, wgu.at[:, pl.ds(0, hid)]), load(wu, wgu.at[:, pl.ds(hid, hid)]),
                  load(wd_hbm, wd)]

    routing_in.wait()
    r0, r1 = rt[0:1, :], rt[1:2, :]
    row_e = lax.broadcasted_iota(jnp.int32, (128, toks), 0)
    member_t = (r0 == row_e) | (r1 == row_e)
    earlier = (lax.broadcasted_iota(jnp.int32, (toks, toks), 0)
               < lax.broadcasted_iota(jnp.int32, (toks, toks), 1))
    place_t = contract(member_t.astype(F32).astype(BF16), earlier.astype(F32).astype(BF16),
                       ((1,), (0,)))
    place_t = jnp.where(member_t, place_t, -1000.0)[:n_exp]
    member_t = member_t[:n_exp]
    info[z] = place_t
    slot_id = lax.broadcasted_iota(jnp.int32, (cap, toks), 0).astype(F32)

    raw_in[0].wait()
    pl.semaphore_wait(barrier, 4 + is_mid.astype(jnp.int32))

    def group_of(kind):
        return RAW if kind[0] == "raw" else SMALL

    def along(kind, ref, s):
        if s == 0:
            send((kind, "pair"), ref, ref, group_of(kind), ep=ep_of(z_pair), arrival=(kind, 1))

            only(is_mid, "mid", lambda: send((kind, "mid"), ref, ref, group_of(kind),
                                             ep=ep_of(z_mid), arrival=(kind, 2)))
        elif s == 1:
            send((kind, "mid1"), ref, ref, group_of(kind), ep=ep_of(z_mid), arrival=(kind, 3))
        else:
            send((kind, "out", s), ref, ref, group_of(kind), ep=ep_of(z_pair), arrival=(kind, s))

    along("info", info.at[z], 0)
    along(("raw", 0), raw.at[z, 0], 0)
    raw_in[1].wait()
    along(("raw", 1), raw.at[z, 1], 0)
    pl.semaphore_signal(ready, inc=1, device_id=(e, p_x), device_id_type=MESH)
    for copy in raw_in[2:]:
        copy.wait()

    def wide():
        for a in (0, 1):
            send(("wide", a), other_x.at[a], raw_x.at[a], RAW, ep=ep_of(z_pair))


    def parts_of(s, a):
        plane = planes[s]
        own = [(("raw", a), raw.at[plane, a])]
        if a == 0:
            return [("info", info.at[plane])] + own
        return own + [("gall", gall.at[ep_of(plane)])]

    def pass_on(s, a):
        for kind, ref in parts_of(s, a):
            landed((kind, s), ref)
            along(kind, ref, s)

    def settle(s, a):
        for kind, ref in parts_of(s, a):
            landed((kind, s), ref)

    def chosen(s, x):
        return (info[planes[s], pl.ds(x, 1), :] == slot_id).astype(F32).astype(BF16)

    def core(key, a, block, src):
        ref = arr_a.at[block, src, a]
        send((key, a), ref, ref, TO_CORE, tp=p_core, arrival=("c", key[1], a))

    def pick(s, a, diagonal=1):
        plane = planes[s]
        src = ep_of(plane)
        if s and a:
            send(("gy", s), gall.at[src], gall.at[src], SMALL, ep=e_y)
        if s:
            picks = jnp.concatenate([chosen(s, e_y), chosen(s, e)], axis=0)
        else:
            picks = chosen(s, e_y)
        rows = contract(picks, raw[plane, a], ((1,), (0,))).astype(BF16)
        ysa[plane, a] = rows[:cap]
        there = arr_a.at[p, src, a]
        send(("y", s, a), ysa.at[plane, a], there, TO_Y, ep=e_y)
        if s:
            if diagonal:
                send(("x", s, 1, a), ysa.at[plane, a], there, TO_X, ep=e_y, tp=p_x)
            arr_a[p, src, a] = rows[cap:]
            send(("x", s, 0, a), there, there, TO_X, tp=p_x)
            core(("c", s, 0), a, p, src)
        else:
            ysx[a] = contract(picks, other_x[a], ((1,), (0,))).astype(BF16)
            send(("yx", a), ysx.at[a], arr_a.at[p_x, src, a], TO_Y, ep=e_y, arrival=("y", 0, a))

    def pick_wide(a):
        src = ep_of(z_pair)
        if a == 0:
            send(("gy", 1), gall.at[src], gall.at[src], SMALL, ep=e_y)
        picks = jnp.concatenate([chosen(1, e_y), chosen(1, e)], axis=0)
        for i, (block, source) in enumerate(((p, raw.at[z_pair, a]), (p_x, raw_x.at[a]))):
            if i:
                landed(("wide", a), raw_x.at[a])
            rows = contract(picks, source[...], ((1,), (0,))).astype(BF16)
            buffer = ysw.at[a] if i else ysa.at[z_pair, a]
            buffer[...] = rows[:cap]
            send(("yw", a, i), buffer, arr_a.at[block, src, a], TO_Y, ep=e_y, arrival=("yw", a))
            arr_a[block, src, a] = rows[cap:]
            core(("cw"[i], 1, 0), a, block, src)

    def from_y_wide(a):
        src = ep_of(z_pair, 1)
        landed(("yw", a), ysx)
        core(("c", 1, 1), a, p, src)
        core(("c2", 1, 1), a, p_x, src)

    def from_y(s, a, diagonal=1):
        src = ep_of(planes[s], 1)
        landed(("y", s, a), arr_a.at[p, src, a] if s else ysx)
        if not diagonal:
            send(("x", s, 1, a), arr_a.at[p, src, a], arr_a.at[p, src, a], TO_X, tp=p_x)
        core(("c", s, 1), a, p, src)
        if s == 0:
            core(("c2", s, 1), a, p_x, src)

    def from_x(s, h, a):
        src = ep_of(planes[s], h)
        landed(("x", s, h, a), arr_a.at[p_x, src, a])
        core(("c2", s, h), a, p_x, src)

    def gathered(s, a):
        landed(("c", s, a), arr_a.at[0, pl.ds(0, 2)] if s else ysx)

    def compute_a(s):
        gathered(s, 0)
        pair = pl.ds(planes[s] * 2, 2)
        pre = jnp.zeros((two, 2 * hid), F32)
        for b in range(n_tp):
            c = slice(b * fb, (b + 1) * fb)
            pre = pre + contract(arr_a[b, pair, 0].reshape(two, fb), wgu[c, :], ((1,), (0,)))
        pre_gate, pre_up = pre[:, :hid], pre[:, hid:]
        activated, slope = silu_parts(pre_gate)
        mid[s, 0] = activated
        mid[s, 1] = pre_up * slope
        mid[s, 2] = (activated * pre_up).astype(BF16).astype(F32)

    def gates(s):
        base = planes[s] * 2
        landed(("gy", s), gall.at[ep_of(planes[s], 1)])
        for i in (0, 1):
            row = gall[base + i, pl.ds(e, 1), :]
            hit = gall[base + i, pl.ds(n_exp + e, 1), :] == slot_id
            column = jnp.sum(jnp.where(hit, row, 0.0), axis=1, keepdims=True)
            mid[s, 3, i * cap:(i + 1) * cap] = jnp.broadcast_to(column, (cap, hid))

    def compute_b(s):
        plane = planes[s]
        base = plane * 2
        gathered(s, 1)
        pair = pl.ds(base, 2)
        here = pl.ds(pl.multiple_of(base * cap, two), two)
        back = jnp.zeros((two, hid), F32)
        for b in range(n_tp):
            c = slice(b * fb, (b + 1) * fb)
            back = back + contract(arr_a[b, pair, 1].reshape(two, fb), wd[:, c], ((1,), (1,)))
        gate = mid[s, 3]
        hidden = mid[s, 2]
        scaled = gate * back
        grads = jnp.concatenate([(scaled * mid[s, 1]).astype(BF16),
                                 (scaled * mid[s, 0]).astype(BF16)], axis=1)
        for i, b in ((1, p_both), (0, p_core)):
            wb = wgu[pl.ds(pl.multiple_of(b * fb, 128), fb), :]
            part[b, pair] = contract(grads, wb, ((1,), (1,))).astype(BF16).reshape(2, cap, fb)
            send(("pc", s, i), part.at[b, pair], pc.at[i, pair], BACK, tp=p_core)
        ggb[plane] = contract(jnp.ones((8, hid), F32), hidden * back, ((1,), (1,)),
                              lax.Precision.HIGHEST)
        send(("ggc", s), ggb.at[plane], ggc.at[plane], SMALL, tp=p_core)
        for b in (p_x, p):
            wb = wgu[pl.ds(pl.multiple_of(b * fb, 128), fb), :]
            part[b, pair] = contract(grads, wb, ((1,), (1,))).astype(BF16).reshape(2, cap, fb)
        gp[here, :] = grads
        sh[here, :] = (gate * hidden).astype(BF16)

    def gate_home(s):
        plane = planes[s]
        landed(("ggc", s), ggc.at[plane])
        ggs[plane] = ggb[plane] + ggc[plane]
        for h in (0, 1):
            for far, tp in ((0, p), (1, p_x)):
                if s == 0 and h == 0 and far == 0:
                    ggh[e, x_me] = ggs[plane]
                else:
                    send(("ggh", s, h, far), ggs.at[plane], ggh.at[e, x_me], SMALL,
                         ep=ep_of(plane, h), tp=tp, arrival="ggh" if s or h else "ggh2")

    def to_x(s):
        pair = pl.ds(planes[s] * 2, 2)
        landed(("pc", s, 1), pc.at[1, pair])
        xs[pair] = (part[p_x, pair].astype(F32) + pc[1, pair].astype(F32)).astype(BF16)
        for h in ((0, 1) if s else (1, 0)):
            src = ep_of(planes[s], h)
            send(("xs", s, h), xs.at[src], xr.at[src], BACK, tp=p_x)
        landed(("pc", s, 0), pc.at[0, pair])

    def to_home(s, h):
        other = ep_of(planes[s], h)
        landed(("xs", s, h), xr.at[other])
        fin[other] = (part[p, other].astype(F32) + pc[0, other].astype(F32)
                      + xr[other].astype(F32)).astype(BF16)
        if s or h:
            send(("fin", s, h), fin.at[other], home.at[e], HOME, ep=other, arrival="fin")
        else:
            home[e] = fin[e]

    def in_block(b):
        rows = arr_a[b, :, 0].reshape(n_ep * cap, fb)
        sums = contract(gp[...], rows, ((0,), (0,)))
        c = slice(b * fb, (b + 1) * fb)
        o_gate[c, :] = jnp.transpose(sums[:hid]).astype(BF16)
        o_up[c, :] = jnp.transpose(sums[hid:]).astype(BF16)
        nb[0:1, c] = jnp.sum(sums[:hid] * sums[:hid], axis=0, keepdims=True)
        nb[1:2, c] = jnp.sum(sums[hid:] * sums[hid:], axis=0, keepdims=True)

    def down():
        dn = jnp.zeros((hid, 1), F32)
        for b in range(n_tp):
            sums = contract(sh[...], arr_a[b, :, 1].reshape(n_ep * cap, fb), ((0,), (0,)))
            o_down[:, b * fb:(b + 1) * fb] = sums.astype(BF16)
            dn = dn + jnp.sum(sums * sums, axis=1, keepdims=True)
        o_dnorm[...] = jnp.transpose(jnp.broadcast_to(dn, (hid, 128)))[0:1, :]

    pick(0, 0)
    pick(0, 1)

    for copy in full_in[:2]:
        copy.wait()
    logits_t = contract(rw[...], tok[...], ((1,), (1,)))
    score_t = jnp.where(member_t, jax.nn.sigmoid(logits_t), 0.0)
    score_sum = jnp.sum(score_t, axis=0, keepdims=True)
    gating_t = score_t / score_sum
    gall[e, 0:n_exp] = gating_t
    gall[e, n_exp:2 * n_exp] = place_t
    along("gall", gall.at[e], 0)
    only(is_edge, "edge", wide)
    send(("gy", 0), gall.at[e], gall.at[e], SMALL, ep=e_y)
    for x in range(n_exp):
        sel[x] = (place_t[x:x + 1, :] == slot_id).astype(F32).astype(BF16)
    full_in[2].wait()
    for a, ref in enumerate((tok, cot)):
        rows = contract(sel[e], ref[...], ((1,), (0,))).astype(BF16)
        for b in range(n_tp):
            arr_a[b, e, a] = rows[:, b * fb:(b + 1) * fb]
    for copy in weights_in:
        copy.wait()
    pl.semaphore_wait(ready, 1)

    def router():
        landed("ggh", ggh.at[pl.ds(0, n_exp - 1)])
        landed("ggh2", ggh.at[0, 0])
        gts[0:n_exp, :] = ggh[:, 0, 0, :] + ggh[:, 1, 0, :]
        gts[...] = jnp.transpose(gts[...])
        mine = gts[pl.ds(pl.multiple_of(y * cap, 8), cap), :]
        got_t = jnp.concatenate([jnp.sum(jnp.where(
            place_t[x:x + 1, :] == slot_id, mine[:, x:x + 1], 0.0), axis=0, keepdims=True)
            for x in range(n_exp)], axis=0)
        for k, r in enumerate((r0, r1)):
            o_gg[k:k + 1, :] = jnp.sum(jnp.where(r == row_e[:n_exp], got_t, 0.0), axis=0, keepdims=True)
        weighted = jnp.sum(gating_t * got_t, axis=0, keepdims=True)
        grad_logits = jnp.where(member_t, (got_t - weighted) / score_sum * score_t * (1.0 - score_t),
                                0.0).astype(BF16)
        gl[...] = grad_logits
        rp[...] = contract(grad_logits, tok[...], ((1,), (0,)))
        span = width // n_ep
        for s in (3, 2, 1, 0):
            for h in (1, 0):
                if s or h:
                    other = ep_of(planes[s], h)
                    send(("rr", s, h), rp.at[:, pl.ds(pl.multiple_of(other * span, 128), span)],
                         rr.at[e], SMALL, ep=other, arrival="rr")
        rr[e] = rp[:, pl.ds(pl.multiple_of(e * span, 128), span)]

    def mid_plane():
        pass_on(1, 0)
        pass_on(2, 0)
        pick(2, 0)
        pass_on(1, 1)
        pass_on(2, 1)
        pick(2, 1)
        from_y(0, 0)
        from_y(0, 1)
        compute_a(0)
        pass_on(3, 0)
        pick(3, 0)
        gates(0)
        compute_b(0)
        from_x(2, 0, 0)
        from_y(2, 0)
        from_x(2, 1, 0)
        gate_home(0)
        pass_on(3, 1)
        pick(3, 1)
        pick_wide(0)
        pick_wide(1)
        from_x(2, 0, 1)
        from_y(2, 1)
        gates(2)
        from_x(2, 1, 1)
        compute_a(2)
        compute_b(2)
        from_x(3, 0, 0)
        from_y(3, 0)
        from_x(3, 1, 0)
        gate_home(2)
        to_x(2)
        to_x(0)
        compute_a(3)
        from_x(3, 0, 1)
        from_y(3, 1)
        gates(3)
        from_x(3, 1, 1)
        compute_b(3)
        to_home(2, 0)
        from_y_wide(0)
        to_home(2, 1)
        gate_home(3)
        to_x(3)
        compute_a(1)
        gates(1)
        from_y_wide(1)
        compute_b(1)
        to_home(3, 0)
        in_block(0)
        in_block(1)
        to_home(3, 1)
        gate_home(1)
        to_x(1)
        in_block(2)
        in_block(3)
        send("nbc", nb, nc, SMALL, tp=p_core)
        down()
        landed("nbc", nc)
        nc[...] = nb[...] + nc[...]
        send("nbx", nc, nx, SMALL, tp=p_x)
        to_home(1, 0)
        to_home(1, 1)
        router()
        to_home(0, 1)
        to_home(0, 0)

    def edge_plane():
        settle(1, 0)
        pick(1, 0)
        settle(1, 1)
        pick(1, 1)
        settle(2, 0)
        pick(2, 0, 0)
        from_y(0, 0)
        from_y(0, 1)
        gates(0)
        compute_a(0)
        from_y(1, 0)
        settle(2, 1)
        pick(2, 1)
        compute_b(0)
        from_x(1, 0, 0)
        from_x(1, 1, 0)
        from_y(1, 1)
        from_x(1, 0, 1)
        from_x(1, 1, 1)
        from_y(2, 0, 0)
        gates(1)
        compute_a(1)
        settle(3, 0)
        pick(3, 0)
        compute_b(1)
        settle(3, 1)
        pick(3, 1)
        from_x(2, 0, 0)
        from_y(2, 1)
        from_x(2, 0, 1)
        from_x(2, 1, 0)
        gate_home(0)
        gate_home(1)
        to_x(1)
        gates(2)
        from_x(2, 1, 1)
        compute_a(2)
        compute_b(2)
        from_y(3, 0)
        from_x(3, 0, 0)
        from_x(3, 1, 0)
        gates(3)
        compute_a(3)
        gate_home(2)
        to_x(2)
        from_y(3, 1)
        from_x(3, 0, 1)
        from_x(3, 1, 1)
        compute_b(3)
        to_home(1, 0)
        in_block(0)
        in_block(1)
        gate_home(3)
        to_x(3)
        to_x(0)
        to_home(1, 1)
        to_home(2, 0)
        in_block(2)
        to_home(2, 1)
        in_block(3)
        send("nbc", nb, nc, SMALL, tp=p_core)
        down()
        to_home(3, 0)
        landed("nbc", nc)
        nc[...] = nb[...] + nc[...]
        send("nbx", nc, nx, SMALL, tp=p_x)
        to_home(3, 1)
        router()
        to_home(0, 1)
        to_home(0, 0)

    only(is_mid, "mid", mid_plane)
    only(is_edge, "edge", edge_plane)


    landed("nbx", nx)
    o_norm[...] = nc[...] + nx[...]
    landed("fin", home.at[pl.ds(0, n_ep - 1)])
    landed("rr", rr.at[pl.ds(0, n_ep - 1)])
    total = rr[0]
    for x in range(1, n_ep):
        total = total + rr[x]
    o_gr[...] = total
    o_rnorm[...] = jnp.sum(total * total, axis=0, keepdims=True)
    router_term = contract(gl[...], rw[:, cols], ((0,), (0,)))
    all_sel = sel[...].reshape(n_exp * cap, toks)
    o_tok[...] = (contract(all_sel, home[...].reshape(n_exp * cap, fb), ((0,), (0,)))
                  + router_term).astype(BF16)
    def drain(name):
        for group in range(SMALL + 1):
            count = sum(n for (where, _), (g, n) in sends.items()
                        if g == group and where in ("all", name))
            if group == SMALL:
                d = next(d for d in (4, 2, 1) if count % d == 0)
                whole = mid.at[pl.ds(0, d), 0, pl.ds(0, count // d * n_exp)]
            else:
                d, k, j = next((d, k, j) for d in range(1, n_tp + 1) for j in (1, 2)
                               for k in range(1, n_ep + 1) if d * k * j == count)
                whole = arr_a.at[pl.ds(0, d), pl.ds(0, k), pl.ds(0, j)]
            transfer(group, "fin", whole, whole).wait_send()

    only(is_edge, "edge", lambda: drain("edge"))
    only(is_mid, "mid", lambda: drain("mid"))


def flush(*refs):
    sem = refs[-1]
    copies = [pltpu.make_async_copy(refs[i], refs[9 + i], sem.at[i]) for i in range(9)]
    for copy in copies:
        copy.start()
    for copy in copies:
        copy.wait()


def fused(tokens, cotangent, routing, router_weight, gate_weight, up_weight, down_weight):
    n_ep, n_tp = lax.axis_size("ep"), lax.axis_size("tp")
    toks, width = tokens.shape
    n_exp = router_weight.shape[1]
    cap = max(2, 2 * toks * routing.shape[1] // n_exp)
    hid = gate_weight.shape[2]
    fb = width // n_tp
    two = 2 * cap
    slots = n_ep * cap
    span = width // n_ep
    results = [
        ((toks, fb), BF16),
        ((routing.shape[1], toks), F32),
        ((n_exp, span), F32),
        ((width, hid), BF16),
        ((width, hid), BF16),
        ((hid, width), BF16),
        ((2, width), F32),
        ((1, hid), F32),
        ((1, span), F32),
    ]
    vmem = pl.BlockSpec(memory_space=pltpu.VMEM)
    hbm = pl.BlockSpec(memory_space=pltpu.HBM)
    outs = pl.pallas_call(
        functools.partial(kernel, n_ep, n_tp, cap),
        out_shape=[pltpu.VMEM(shape, dtype) for shape, dtype in results],
        in_specs=[hbm] * 7,
        out_specs=[vmem] * 9,
        scratch_shapes=[
            pltpu.VMEM((routing.shape[1], toks), jnp.int32),
            pltpu.VMEM((n_exp, width), BF16),
            pltpu.VMEM((toks, width), BF16),
            pltpu.VMEM((toks, width), BF16),
            pltpu.VMEM((width, 2 * hid), BF16),
            pltpu.VMEM((hid, width), BF16),
            pltpu.VMEM((n_exp, cap, toks), BF16),
            pltpu.VMEM((n_ep // 2, 2, toks, fb), BF16),
            pltpu.VMEM((n_ep // 2, n_exp, toks), F32),
            pltpu.VMEM((2, toks, fb), BF16),
            pltpu.VMEM((2, toks, fb), BF16),
            pltpu.VMEM((n_ep // 2, 2, cap, fb), BF16),
            pltpu.VMEM((2, cap, fb), BF16),
            pltpu.VMEM((2, cap, fb), BF16),
            pltpu.VMEM((n_tp, n_ep, 2, cap, fb), BF16),
            pltpu.VMEM((n_ep, 2 * n_exp, toks), F32),
            pltpu.VMEM((n_ep // 2, 4, two, hid), F32),
            pltpu.VMEM((n_tp, n_ep, cap, fb), BF16),
            pltpu.VMEM((2, n_ep, cap, fb), BF16),
            pltpu.VMEM((n_ep, cap, fb), BF16),
            pltpu.VMEM((n_ep, cap, fb), BF16),
            pltpu.VMEM((n_ep, cap, fb), BF16),
            pltpu.VMEM((n_exp, cap, fb), BF16),
            pltpu.VMEM((slots, 2 * hid), BF16),
            pltpu.VMEM((slots, hid), BF16),
            pltpu.VMEM((n_ep // 2, 8, two), F32),
            pltpu.VMEM((n_ep // 2, 8, two), F32),
            pltpu.VMEM((n_ep // 2, 8, two), F32),
            pltpu.VMEM((n_exp, 2, 8, two), F32),
            pltpu.VMEM((two, toks), F32),
            pltpu.VMEM((2, width), F32),
            pltpu.VMEM((2, width), F32),
            pltpu.VMEM((2, width), F32),
            pltpu.VMEM((n_exp, toks), BF16),
            pltpu.VMEM((n_exp, width), F32),
            pltpu.VMEM((n_ep, n_exp, span), F32),
            pltpu.SemaphoreType.DMA((11,)),
            pltpu.SemaphoreType.DMA((SMALL + 1,)),
            pltpu.SemaphoreType.DMA((80,)),
            pltpu.SemaphoreType.REGULAR,
        ],
        compiler_params=pltpu.CompilerParams(
            collective_id=0, has_side_effects=True, vmem_limit_bytes=40 << 20
        ),
    )(*[pltpu.with_memory_space_constraint(v, pltpu.HBM)
        for v in (tokens, cotangent, routing.T, router_weight.T,
                  gate_weight[0], up_weight[0], down_weight[0])])
    outs = pl.pallas_call(
        flush,
        out_shape=[jax.ShapeDtypeStruct(shape, dtype) for shape, dtype in results],
        in_specs=[vmem] * 9,
        out_specs=[hbm] * 9,
        scratch_shapes=[pltpu.SemaphoreType.DMA((9,))],
    )(*[pltpu.with_memory_space_constraint(v, pltpu.VMEM) for v in outs])
    o_tok, o_gg, o_gr, o_gate, o_up, o_down, o_norm, o_dnorm, o_rnorm = outs
    return (o_tok, o_gg.T, o_gr.T, o_gate[None], o_up[None], o_down[None], o_norm[None],
            o_dnorm, o_rnorm[0])


def shards(tokens, cotangent, routing, router_weight, gate_weight, up_weight, down_weight):
    n_ep, n_tp = lax.axis_size("ep"), lax.axis_size("tp")
    toks, width = tokens.shape
    n_exp = router_weight.shape[1]
    cap = max(2, 2 * toks * routing.shape[1] // n_exp)
    fits = (
        n_tp == 4 and n_ep == 8 and n_ep == n_exp
        and 2 * cap == toks == 128 and gate_weight.shape[2] == 128
        and routing.shape[1] == 2 and width % (128 * 8) == 0
    )
    form = fused if fits else general
    return form(tokens, cotangent, routing, router_weight, gate_weight, up_weight, down_weight)


def solution(mesh):
    in_specs = (
        P("ep", None),
        P("ep", None),
        P("ep", None),
        P(),
        P("ep", None, "tp"),
        P("ep", None, "tp"),
        P("ep", "tp", None),
    )
    out_specs = (
        P("ep", "tp"),
        P("ep", None),
        P("ep", None),
        P("ep", None, "tp"),
        P("ep", None, "tp"),
        P("ep", "tp", None),
        P("ep", None, None),
        P("ep", "tp"),
        P("ep"),
    )
    return jax.shard_map(shards, mesh=mesh, in_specs=in_specs, out_specs=out_specs, check_vma=False)
```

```python
import functools
import math

import jax
import jax.numpy as jnp
from jax import lax
from jax.experimental import pallas as pl
from jax.experimental.pallas import tpu as pltpu
from jax.sharding import PartitionSpec as P


def silu_parts(pre_gate):
    sigmoid_gate = jax.nn.sigmoid(pre_gate)
    return (pre_gate * sigmoid_gate, sigmoid_gate * (1.0 + pre_gate * (1.0 - sigmoid_gate)))


def slot_layout(routing, experts_all, capacity):
    tok_count, top_count = routing.shape
    flat_expert = routing.reshape(-1)
    one_hot = (flat_expert[:, None] == jnp.arange(experts_all, dtype=jnp.int32)[None, :]).astype(
        jnp.int32
    )
    earlier = jnp.cumsum(one_hot, axis=0) - one_hot
    within = jnp.sum(earlier * one_hot, axis=1)
    position = flat_expert * capacity + within
    vacant = jnp.full((experts_all * capacity,), tok_count * top_count, jnp.int32)
    return (vacant.at[position].set(jnp.arange(tok_count * top_count, dtype=jnp.int32)), position)


def general(tokens, cotangent, routing, router_weight, gate_weight, up_weight, down_weight):
    tok_count, model_width = tokens.shape
    top_count = routing.shape[1]
    experts_all = router_weight.shape[1]
    expert_local = gate_weight.shape[0]
    ep_size = lax.axis_size("ep")
    tp_size = lax.axis_size("tp")
    tp_index = lax.axis_index("tp")
    slice_width = model_width // tp_size
    capacity = max(2, 2 * tok_count * top_count // experts_all)
    arrived = ep_size * capacity
    logits = jnp.dot(tokens, router_weight, preferred_element_type=jnp.float32)
    picked = (
        routing[:, :, None] == jnp.arange(experts_all, dtype=jnp.int32)[None, None, :]
    ).astype(jnp.float32)
    scores = jax.nn.sigmoid(jnp.einsum("tke,te->tk", picked, logits))
    score_sum = jnp.sum(scores, axis=1, keepdims=True)
    gating = scores / score_sum
    assignment, position = slot_layout(routing, experts_all, capacity)
    source_row = assignment // top_count
    padded_tokens = jnp.concatenate([tokens, jnp.zeros((1, model_width), tokens.dtype)], axis=0)
    padded_cotangent = jnp.concatenate(
        [cotangent, jnp.zeros((1, model_width), cotangent.dtype)], axis=0
    )
    padded_gating = jnp.concatenate([gating.reshape(-1), jnp.zeros((1,), jnp.float32)])
    sent_gating = padded_gating[assignment].reshape(experts_all, capacity)
    own_tokens = lax.dynamic_slice_in_dim(padded_tokens, tp_index * slice_width, slice_width, 1)
    own_cotangent = lax.dynamic_slice_in_dim(
        padded_cotangent, tp_index * slice_width, slice_width, 1
    )
    part_tokens, part_cotangent = (
        lax.all_to_all(
            own_tokens[source_row].reshape(experts_all, capacity, slice_width),
            "ep",
            split_axis=0,
            concat_axis=0,
            tiled=True,
        ),
        lax.all_to_all(
            own_cotangent[source_row].reshape(experts_all, capacity, slice_width),
            "ep",
            split_axis=0,
            concat_axis=0,
            tiled=True,
        ),
    )
    got_tokens, got_cotangent = (
        lax.all_gather(part_tokens, "tp", axis=2, tiled=True),
        lax.all_gather(part_cotangent, "tp", axis=2, tiled=True),
    )
    got_gating = lax.all_to_all(sent_gating, "ep", split_axis=0, concat_axis=0, tiled=True)

    def by_expert(values):
        shaped = values.reshape((ep_size, expert_local) + values.shape[1:])
        return jnp.moveaxis(shaped, 1, 0).reshape((expert_local, arrived) + values.shape[2:])

    def by_source(values):
        shaped = values.reshape((expert_local, ep_size, capacity) + values.shape[2:])
        return jnp.moveaxis(shaped, 1, 0).reshape(
            (ep_size * expert_local, capacity) + values.shape[2:]
        )

    rows_in = by_expert(got_tokens)
    cot_rows = by_expert(got_cotangent)
    slot_gating = by_expert(got_gating)[:, :, None]
    pre_gate = jnp.einsum("lrd,ldf->lrf", rows_in, gate_weight, preferred_element_type=jnp.float32)
    pre_up = jnp.einsum("lrd,ldf->lrf", rows_in, up_weight, preferred_element_type=jnp.float32)
    activated, silu_slope = silu_parts(pre_gate)
    hidden = (activated * pre_up).astype(jnp.bfloat16)
    back_raw = jnp.einsum("lrd,lfd->lrf", cot_rows, down_weight, preferred_element_type=jnp.float32)
    hidden_wide = hidden.astype(jnp.float32)
    gate_partial = jnp.sum(hidden_wide * back_raw, axis=2)
    scaled_back = slot_gating * back_raw
    grad_pre_gate = (scaled_back * pre_up * silu_slope).astype(jnp.bfloat16)
    grad_pre_up = (scaled_back * activated).astype(jnp.bfloat16)
    scaled_hidden = (slot_gating * hidden_wide).astype(jnp.bfloat16)
    gate_sum = jnp.einsum(
        "lrd,lrf->ldf", rows_in, grad_pre_gate, preferred_element_type=jnp.float32
    )
    up_sum = jnp.einsum("lrd,lrf->ldf", rows_in, grad_pre_up, preferred_element_type=jnp.float32)
    down_sum = jnp.einsum(
        "lrf,lrd->lfd", scaled_hidden, cot_rows, preferred_element_type=jnp.float32
    )
    down_norms = jnp.sum(down_sum * down_sum, axis=2)
    back_partial = jnp.einsum(
        "lrf,ldf->lrd", grad_pre_gate, gate_weight, preferred_element_type=jnp.float32
    ) + jnp.einsum("lrf,ldf->lrd", grad_pre_up, up_weight, preferred_element_type=jnp.float32)
    back_rounded = back_partial.astype(jnp.bfloat16)
    slot_values = (
        lax.psum_scatter(back_rounded, "tp", scatter_dimension=2, tiled=True)
        .astype(jnp.float32)
        .astype(jnp.bfloat16)
    )
    gating_total, gate_rows, up_rows = lax.psum(
        (gate_partial, jnp.sum(gate_sum * gate_sum, axis=2), jnp.sum(up_sum * up_sum, axis=2)), "tp"
    )
    home_values = lax.all_to_all(
        by_source(slot_values), "ep", split_axis=0, concat_axis=0, tiled=True
    )
    home_gating = lax.all_to_all(
        by_source(gating_total), "ep", split_axis=0, concat_axis=0, tiled=True
    )
    flat_values = home_values.reshape(experts_all * capacity, slice_width)
    token_terms = (
        flat_values[position].reshape(tok_count, top_count, slice_width).astype(jnp.float32)
    )
    grad_gating = home_gating.reshape(-1)[position].reshape(tok_count, top_count)
    weighted = jnp.sum(gating * grad_gating, axis=1, keepdims=True)
    grad_scores = (grad_gating - weighted) / score_sum
    grad_chosen = grad_scores * scores * (1.0 - scores)
    grad_logits = jnp.einsum("tk,tke->te", grad_chosen, picked).astype(jnp.bfloat16)
    router_slice = lax.dynamic_slice_in_dim(router_weight, tp_index * slice_width, slice_width, 0)
    router_term = jnp.einsum(
        "te,de->td", grad_logits, router_slice, preferred_element_type=jnp.float32
    )
    grad_tokens = (jnp.sum(token_terms, axis=1) + router_term).astype(jnp.bfloat16)
    grad_router = lax.psum_scatter(
        jnp.einsum("td,te->de", tokens, grad_logits, preferred_element_type=jnp.float32),
        "ep",
        scatter_dimension=0,
        tiled=True,
    )
    router_norms = jnp.sum(grad_router * grad_router, axis=1)
    in_norms = jnp.stack([gate_rows, up_rows], axis=1)
    return (
        grad_tokens,
        grad_gating,
        grad_router,
        gate_sum.astype(jnp.bfloat16),
        up_sum.astype(jnp.bfloat16),
        down_sum.astype(jnp.bfloat16),
        in_norms,
        down_norms,
        router_norms,
    )


MESH = pl.DeviceIdType.MESH
RAW, TO_Y, TO_X, TO_CORE, BACK, HOME, SMALL = range(7)
F32 = jnp.float32
BF16 = jnp.bfloat16


def contract(a, b, dims, precision=None):
    return lax.dot_general(
        a, b, ((dims[0], dims[1]), ((), ())), precision=precision, preferred_element_type=F32
    )


def flipped(index, mask, bits):
    out = index
    for bit in range(bits):
        if (mask >> bit) & 1:
            out = out + (1 << bit) * (1 - 2 * ((index // (1 << bit)) % 2))
    return out


def kernel(n_ep, n_tp, cap,
           tok_hbm, cot_hbm, rt_hbm, rw_hbm, wg, wu, wd_hbm,
           o_tok, o_gg, o_gr, o_gate, o_up, o_down, o_norm, o_dnorm, o_rnorm,
           rt, rw, tok, cot, wgu, wd, sel, raw, info, other_x, raw_x, ysa, ysx, ysw, arr_a, gall, mid, part, pc, xs, xr,
           fin, home, gp, sh, ggb, ggc, ggs, ggh, gts, nb, nc, nx, gl, rp, rr, lsem, ssem, rsem, ready):
    e = lax.axis_index("ep")
    p = lax.axis_index("tp")
    z, y = e // 2, e % 2
    x_me = p // 2
    toks, width = tok.shape
    n_exp = rw.shape[0]
    fb = width // n_tp
    hid = wd.shape[0]
    two = 2 * cap
    p_core, p_x, p_both = (flipped(p, m, 2) for m in (1, 2, 3))
    z_pair, z_mid = flipped(z, 1, 1), 3 - z
    is_mid = (z == 1) | (z == 2)
    is_edge = jnp.logical_not(is_mid)
    planes = (z, z_pair, 2 - z // 2, 3 - 3 * (z // 2))
    e_y = z * 2 + 1 - y
    sends, slots, local, branch = {}, {}, [], ["all"]

    def ep_of(plane, h=0):
        return plane * 2 + (y + h) % 2

    def receiver(arrival):
        return slots.setdefault(arrival, len(slots))

    def transfer(group, arrival, source, dest, ep=None, tp=None):
        return pltpu.make_async_remote_copy(
            src_ref=source, dst_ref=dest, send_sem=ssem.at[group],
            recv_sem=rsem.at[receiver(arrival)],
            device_id=(e if ep is None else ep, p if tp is None else tp), device_id_type=MESH)

    def send(key, source, dest, group, ep=None, tp=None, arrival=None):
        transfer(group, key if arrival is None else arrival, source, dest, ep, tp).start()
        unit = n_exp * 128 if group == SMALL else cap * fb
        sends[branch[-1], key] = (group, math.prod(source.shape) // unit)

    def only(cond, name, body):
        @pl.when(cond)
        def _():
            branch.append(name)
            body()
            branch.pop()

    def landed(arrival, ref):
        transfer(0, arrival, ref, ref).wait_recv()

    def load(source, dest):
        copy = pltpu.make_async_copy(source, dest, lsem.at[len(local)])
        copy.start()
        local.append(copy)
        return copy

    barrier = pltpu.get_barrier_semaphore()
    pl.semaphore_signal(barrier, inc=1, device_id=(ep_of(z_pair), p), device_id_type=MESH)

    @pl.when(is_mid)
    def _():
        pl.semaphore_signal(barrier, inc=1, device_id=(ep_of(z_mid), p), device_id_type=MESH)

    for ep, tp in ((e_y, p), (e, p_x), (e, p_core)):
        pl.semaphore_signal(barrier, inc=1, device_id=(ep, tp), device_id_type=MESH)
    routing_in = load(rt_hbm, rt)
    cols = pl.ds(pl.multiple_of(p * fb, 128), fb)
    cols_x = pl.ds(pl.multiple_of(p_x * fb, 128), fb)
    raw_in = [load(tok_hbm.at[:, cols], raw.at[z, 0]), load(cot_hbm.at[:, cols], raw.at[z, 1])]
    raw_in += [load(tok_hbm.at[:, cols_x], other_x.at[0]), load(cot_hbm.at[:, cols_x], other_x.at[1])]
    full_in = [load(rw_hbm, rw), load(tok_hbm, tok), load(cot_hbm, cot)]
    weights_in = [load(wg, wgu.at[:, pl.ds(0, hid)]), load(wu, wgu.at[:, pl.ds(hid, hid)]),
                  load(wd_hbm, wd)]

    routing_in.wait()
    r0, r1 = rt[0:1, :], rt[1:2, :]
    row_e = lax.broadcasted_iota(jnp.int32, (128, toks), 0)
    member_t = (r0 == row_e) | (r1 == row_e)
    earlier = (lax.broadcasted_iota(jnp.int32, (toks, toks), 0)
               < lax.broadcasted_iota(jnp.int32, (toks, toks), 1))
    place_t = contract(member_t.astype(F32).astype(BF16), earlier.astype(F32).astype(BF16),
                       ((1,), (0,)))
    place_t = jnp.where(member_t, place_t, -1000.0)[:n_exp]
    member_t = member_t[:n_exp]
    info[z] = place_t
    slot_id = lax.broadcasted_iota(jnp.int32, (cap, toks), 0).astype(F32)

    raw_in[0].wait()
    pl.semaphore_wait(barrier, 4 + is_mid.astype(jnp.int32))

    def group_of(kind):
        return RAW if kind[0] == "raw" else SMALL

    def along(kind, ref, s):
        if s == 0:
            send((kind, "pair"), ref, ref, group_of(kind), ep=ep_of(z_pair), arrival=(kind, 1))

            only(is_mid, "mid", lambda: send((kind, "mid"), ref, ref, group_of(kind),
                                             ep=ep_of(z_mid), arrival=(kind, 2)))
        elif s == 1:
            send((kind, "mid1"), ref, ref, group_of(kind), ep=ep_of(z_mid), arrival=(kind, 3))
        else:
            send((kind, "out", s), ref, ref, group_of(kind), ep=ep_of(z_pair), arrival=(kind, s))

    along("info", info.at[z], 0)
    along(("raw", 0), raw.at[z, 0], 0)
    raw_in[1].wait()
    along(("raw", 1), raw.at[z, 1], 0)
    pl.semaphore_signal(ready, inc=1, device_id=(e, p_x), device_id_type=MESH)
    for copy in raw_in[2:]:
        copy.wait()

    def wide():
        for a in (0, 1):
            send(("wide", a), other_x.at[a], raw_x.at[a], RAW, ep=ep_of(z_pair))


    def parts_of(s, a):
        plane = planes[s]
        own = [(("raw", a), raw.at[plane, a])]
        if a == 0:
            return [("info", info.at[plane])] + own
        return own + [("gall", gall.at[ep_of(plane)])]

    def pass_on(s, a):
        for kind, ref in parts_of(s, a):
            landed((kind, s), ref)
            along(kind, ref, s)

    def settle(s, a):
        for kind, ref in parts_of(s, a):
            landed((kind, s), ref)

    def chosen(s, x):
        return (info[planes[s], pl.ds(x, 1), :] == slot_id).astype(F32).astype(BF16)

    def core(key, a, block, src):
        ref = arr_a.at[block, src, a]
        send((key, a), ref, ref, TO_CORE, tp=p_core, arrival=("c", key[1], a))

    def pick(s, a, diagonal=1):
        plane = planes[s]
        src = ep_of(plane)
        if s and a:
            send(("gy", s), gall.at[src], gall.at[src], SMALL, ep=e_y)
        if s:
            picks = jnp.concatenate([chosen(s, e_y), chosen(s, e)], axis=0)
        else:
            picks = chosen(s, e_y)
        rows = contract(picks, raw[plane, a], ((1,), (0,))).astype(BF16)
        ysa[plane, a] = rows[:cap]
        there = arr_a.at[p, src, a]
        send(("y", s, a), ysa.at[plane, a], there, TO_Y, ep=e_y)
        if s:
            if diagonal:
                send(("x", s, 1, a), ysa.at[plane, a], there, TO_X, ep=e_y, tp=p_x)
            arr_a[p, src, a] = rows[cap:]
            send(("x", s, 0, a), there, there, TO_X, tp=p_x)
            core(("c", s, 0), a, p, src)
        else:
            ysx[a] = contract(picks, other_x[a], ((1,), (0,))).astype(BF16)
            send(("yx", a), ysx.at[a], arr_a.at[p_x, src, a], TO_Y, ep=e_y, arrival=("y", 0, a))

    def pick_wide(a):
        src = ep_of(z_pair)
        if a == 0:
            send(("gy", 1), gall.at[src], gall.at[src], SMALL, ep=e_y)
        picks = jnp.concatenate([chosen(1, e_y), chosen(1, e)], axis=0)
        for i, (block, source) in enumerate(((p, raw.at[z_pair, a]), (p_x, raw_x.at[a]))):
            if i:
                landed(("wide", a), raw_x.at[a])
            rows = contract(picks, source[...], ((1,), (0,))).astype(BF16)
            buffer = ysw.at[a] if i else ysa.at[z_pair, a]
            buffer[...] = rows[:cap]
            send(("yw", a, i), buffer, arr_a.at[block, src, a], TO_Y, ep=e_y, arrival=("yw", a))
            arr_a[block, src, a] = rows[cap:]
            core(("cw"[i], 1, 0), a, block, src)

    def from_y_wide(a):
        src = ep_of(z_pair, 1)
        landed(("yw", a), ysx)
        core(("c", 1, 1), a, p, src)
        core(("c2", 1, 1), a, p_x, src)

    def from_y(s, a, diagonal=1):
        src = ep_of(planes[s], 1)
        landed(("y", s, a), arr_a.at[p, src, a] if s else ysx)
        if not diagonal:
            send(("x", s, 1, a), arr_a.at[p, src, a], arr_a.at[p, src, a], TO_X, tp=p_x)
        core(("c", s, 1), a, p, src)
        if s == 0:
            core(("c2", s, 1), a, p_x, src)

    def from_x(s, h, a):
        src = ep_of(planes[s], h)
        landed(("x", s, h, a), arr_a.at[p_x, src, a])
        core(("c2", s, h), a, p_x, src)

    def gathered(s, a):
        landed(("c", s, a), arr_a.at[0, pl.ds(0, 2)] if s else ysx)

    def compute_a(s):
        gathered(s, 0)
        pair = pl.ds(planes[s] * 2, 2)
        pre = jnp.zeros((two, 2 * hid), F32)
        for b in range(n_tp):
            c = slice(b * fb, (b + 1) * fb)
            pre = pre + contract(arr_a[b, pair, 0].reshape(two, fb), wgu[c, :], ((1,), (0,)))
        pre_gate, pre_up = pre[:, :hid], pre[:, hid:]
        activated, slope = silu_parts(pre_gate)
        mid[s, 0] = activated
        mid[s, 1] = pre_up * slope
        mid[s, 2] = (activated * pre_up).astype(BF16).astype(F32)

    def gates(s):
        base = planes[s] * 2
        landed(("gy", s), gall.at[ep_of(planes[s], 1)])
        for i in (0, 1):
            row = gall[base + i, pl.ds(e, 1), :]
            hit = gall[base + i, pl.ds(n_exp + e, 1), :] == slot_id
            column = jnp.sum(jnp.where(hit, row, 0.0), axis=1, keepdims=True)
            mid[s, 3, i * cap:(i + 1) * cap] = jnp.broadcast_to(column, (cap, hid))

    def compute_b(s):
        plane = planes[s]
        base = plane * 2
        gathered(s, 1)
        pair = pl.ds(base, 2)
        here = pl.ds(pl.multiple_of(base * cap, two), two)
        back = jnp.zeros((two, hid), F32)
        for b in range(n_tp):
            c = slice(b * fb, (b + 1) * fb)
            back = back + contract(arr_a[b, pair, 1].reshape(two, fb), wd[:, c], ((1,), (1,)))
        gate = mid[s, 3]
        hidden = mid[s, 2]
        scaled = gate * back
        grads = jnp.concatenate([(scaled * mid[s, 1]).astype(BF16),
                                 (scaled * mid[s, 0]).astype(BF16)], axis=1)
        for i, b in ((1, p_both), (0, p_core)):
            wb = wgu[pl.ds(pl.multiple_of(b * fb, 128), fb), :]
            part[b, pair] = contract(grads, wb, ((1,), (1,))).astype(BF16).reshape(2, cap, fb)
            send(("pc", s, i), part.at[b, pair], pc.at[i, pair], BACK, tp=p_core)
        ggb[plane] = contract(jnp.ones((8, hid), F32), hidden * back, ((1,), (1,)),
                              lax.Precision.HIGHEST)
        send(("ggc", s), ggb.at[plane], ggc.at[plane], SMALL, tp=p_core)
        for b in (p_x, p):
            wb = wgu[pl.ds(pl.multiple_of(b * fb, 128), fb), :]
            part[b, pair] = contract(grads, wb, ((1,), (1,))).astype(BF16).reshape(2, cap, fb)
        gp[here, :] = grads
        sh[here, :] = (gate * hidden).astype(BF16)

    def gate_home(s):
        plane = planes[s]
        landed(("ggc", s), ggc.at[plane])
        ggs[plane] = ggb[plane] + ggc[plane]
        for h in (0, 1):
            for far, tp in ((0, p), (1, p_x)):
                if s == 0 and h == 0 and far == 0:
                    ggh[e, x_me] = ggs[plane]
                else:
                    send(("ggh", s, h, far), ggs.at[plane], ggh.at[e, x_me], SMALL,
                         ep=ep_of(plane, h), tp=tp, arrival="ggh" if s or h else "ggh2")

    def to_x(s):
        pair = pl.ds(planes[s] * 2, 2)
        landed(("pc", s, 1), pc.at[1, pair])
        xs[pair] = (part[p_x, pair].astype(F32) + pc[1, pair].astype(F32)).astype(BF16)
        for h in ((0, 1) if s else (1, 0)):
            src = ep_of(planes[s], h)
            send(("xs", s, h), xs.at[src], xr.at[src], BACK, tp=p_x)

    def to_home(s, h):
        other = ep_of(planes[s], h)
        if h == (0 if s else 1):
            landed(("pc", s, 0), pc.at[0, pl.ds(planes[s] * 2, 2)])
        landed(("xs", s, h), xr.at[other])
        fin[other] = (part[p, other].astype(F32) + pc[0, other].astype(F32)
                      + xr[other].astype(F32)).astype(BF16)
        if s or h:
            send(("fin", s, h), fin.at[other], home.at[e], HOME, ep=other, arrival="fin")
        else:
            home[e] = fin[e]

    def in_block(b):
        rows = arr_a[b, :, 0].reshape(n_ep * cap, fb)
        sums = contract(gp[...], rows, ((0,), (0,)))
        c = slice(b * fb, (b + 1) * fb)
        o_gate[c, :] = jnp.transpose(sums[:hid]).astype(BF16)
        o_up[c, :] = jnp.transpose(sums[hid:]).astype(BF16)
        nb[0:1, c] = jnp.sum(sums[:hid] * sums[:hid], axis=0, keepdims=True)
        nb[1:2, c] = jnp.sum(sums[hid:] * sums[hid:], axis=0, keepdims=True)

    def down():
        dn = jnp.zeros((hid, 1), F32)
        for b in range(n_tp):
            sums = contract(sh[...], arr_a[b, :, 1].reshape(n_ep * cap, fb), ((0,), (0,)))
            o_down[:, b * fb:(b + 1) * fb] = sums.astype(BF16)
            dn = dn + jnp.sum(sums * sums, axis=1, keepdims=True)
        o_dnorm[...] = jnp.transpose(jnp.broadcast_to(dn, (hid, 128)))[0:1, :]

    pick(0, 0)
    pick(0, 1)

    for copy in full_in[:2]:
        copy.wait()
    logits_t = contract(rw[...], tok[...], ((1,), (1,)))
    score_t = jnp.where(member_t, jax.nn.sigmoid(logits_t), 0.0)
    score_sum = jnp.sum(score_t, axis=0, keepdims=True)
    gating_t = score_t / score_sum
    gall[e, 0:n_exp] = gating_t
    gall[e, n_exp:2 * n_exp] = place_t
    along("gall", gall.at[e], 0)
    only(is_edge, "edge", wide)
    send(("gy", 0), gall.at[e], gall.at[e], SMALL, ep=e_y)
    for x in range(n_exp):
        sel[x] = (place_t[x:x + 1, :] == slot_id).astype(F32).astype(BF16)
    full_in[2].wait()
    for a, ref in enumerate((tok, cot)):
        rows = contract(sel[e], ref[...], ((1,), (0,))).astype(BF16)
        for b in range(n_tp):
            arr_a[b, e, a] = rows[:, b * fb:(b + 1) * fb]
    for copy in weights_in:
        copy.wait()
    pl.semaphore_wait(ready, 1)

    def router():
        landed("ggh", ggh.at[pl.ds(0, n_exp - 1)])
        landed("ggh2", ggh.at[0, 0])
        gts[0:n_exp, :] = ggh[:, 0, 0, :] + ggh[:, 1, 0, :]
        gts[...] = jnp.transpose(gts[...])
        mine = gts[pl.ds(pl.multiple_of(y * cap, 8), cap), :]
        got_t = jnp.concatenate([jnp.sum(jnp.where(
            place_t[x:x + 1, :] == slot_id, mine[:, x:x + 1], 0.0), axis=0, keepdims=True)
            for x in range(n_exp)], axis=0)
        for k, r in enumerate((r0, r1)):
            o_gg[k:k + 1, :] = jnp.sum(jnp.where(r == row_e[:n_exp], got_t, 0.0), axis=0, keepdims=True)
        weighted = jnp.sum(gating_t * got_t, axis=0, keepdims=True)
        grad_logits = jnp.where(member_t, (got_t - weighted) / score_sum * score_t * (1.0 - score_t),
                                0.0).astype(BF16)
        gl[...] = grad_logits
        rp[...] = contract(grad_logits, tok[...], ((1,), (0,)))
        span = width // n_ep
        for s in (3, 2, 1, 0):
            for h in (1, 0):
                if s or h:
                    other = ep_of(planes[s], h)
                    send(("rr", s, h), rp.at[:, pl.ds(pl.multiple_of(other * span, 128), span)],
                         rr.at[e], SMALL, ep=other, arrival="rr")
        rr[e] = rp[:, pl.ds(pl.multiple_of(e * span, 128), span)]

    def mid_plane():
        pass_on(1, 0)
        pass_on(2, 0)
        pick(2, 0)
        pass_on(1, 1)
        pass_on(2, 1)
        pick(2, 1)
        from_y(0, 0)
        from_y(0, 1)
        compute_a(0)
        pass_on(3, 0)
        pick(3, 0)
        gates(0)
        compute_b(0)
        from_x(2, 0, 0)
        from_y(2, 0)
        from_x(2, 1, 0)
        gate_home(0)
        pass_on(3, 1)
        pick(3, 1)
        pick_wide(0)
        pick_wide(1)
        from_x(2, 0, 1)
        from_y(2, 1)
        gates(2)
        from_x(2, 1, 1)
        compute_a(2)
        compute_b(2)
        from_x(3, 0, 0)
        from_y(3, 0)
        from_x(3, 1, 0)
        gate_home(2)
        to_x(2)
        to_x(0)
        compute_a(3)
        from_x(3, 0, 1)
        from_y(3, 1)
        gates(3)
        from_x(3, 1, 1)
        compute_b(3)
        to_home(2, 0)
        from_y_wide(0)
        to_home(2, 1)
        gate_home(3)
        to_x(3)
        compute_a(1)
        gates(1)
        from_y_wide(1)
        compute_b(1)
        to_home(3, 0)
        in_block(0)
        in_block(1)
        to_home(3, 1)
        gate_home(1)
        to_x(1)
        in_block(2)
        in_block(3)
        send("nbc", nb, nc, SMALL, tp=p_core)
        down()
        landed("nbc", nc)
        nc[...] = nb[...] + nc[...]
        send("nbx", nc, nx, SMALL, tp=p_x)
        to_home(1, 0)
        to_home(1, 1)
        router()
        to_home(0, 1)
        to_home(0, 0)

    def edge_plane():
        settle(1, 0)
        pick(1, 0)
        settle(1, 1)
        pick(1, 1)
        settle(2, 0)
        pick(2, 0, 0)
        from_y(0, 0)
        from_y(0, 1)
        gates(0)
        compute_a(0)
        from_y(1, 0)
        settle(2, 1)
        pick(2, 1)
        compute_b(0)
        from_x(1, 0, 0)
        from_x(1, 1, 0)
        from_y(1, 1)
        from_x(1, 0, 1)
        from_x(1, 1, 1)
        from_y(2, 0, 0)
        gates(1)
        compute_a(1)
        settle(3, 0)
        pick(3, 0)
        compute_b(1)
        settle(3, 1)
        pick(3, 1)
        from_x(2, 0, 0)
        from_y(2, 1)
        from_x(2, 0, 1)
        from_x(2, 1, 0)
        gate_home(0)
        gate_home(1)
        to_x(1)
        gates(2)
        from_x(2, 1, 1)
        compute_a(2)
        compute_b(2)
        from_y(3, 0)
        from_x(3, 0, 0)
        from_x(3, 1, 0)
        gates(3)
        compute_a(3)
        gate_home(2)
        to_x(2)
        from_y(3, 1)
        from_x(3, 0, 1)
        from_x(3, 1, 1)
        compute_b(3)
        to_home(1, 0)
        in_block(0)
        in_block(1)
        gate_home(3)
        to_x(3)
        to_x(0)
        to_home(1, 1)
        to_home(2, 0)
        in_block(2)
        to_home(2, 1)
        in_block(3)
        send("nbc", nb, nc, SMALL, tp=p_core)
        down()
        to_home(3, 0)
        landed("nbc", nc)
        nc[...] = nb[...] + nc[...]
        send("nbx", nc, nx, SMALL, tp=p_x)
        to_home(3, 1)
        router()
        to_home(0, 1)
        to_home(0, 0)

    only(is_mid, "mid", mid_plane)
    only(is_edge, "edge", edge_plane)


    landed("nbx", nx)
    o_norm[...] = nc[...] + nx[...]
    landed("fin", home.at[pl.ds(0, n_ep - 1)])
    landed("rr", rr.at[pl.ds(0, n_ep - 1)])
    total = rr[0]
    for x in range(1, n_ep):
        total = total + rr[x]
    o_gr[...] = total
    o_rnorm[...] = jnp.sum(total * total, axis=0, keepdims=True)
    router_term = contract(gl[...], rw[:, cols], ((0,), (0,)))
    all_sel = sel[...].reshape(n_exp * cap, toks)
    o_tok[...] = (contract(all_sel, home[...].reshape(n_exp * cap, fb), ((0,), (0,)))
                  + router_term).astype(BF16)
    def drain(name):
        for group in range(SMALL + 1):
            count = sum(n for (where, _), (g, n) in sends.items()
                        if g == group and where in ("all", name))
            if group == SMALL:
                d = next(d for d in (4, 2, 1) if count % d == 0)
                whole = mid.at[pl.ds(0, d), 0, pl.ds(0, count // d * n_exp)]
            else:
                d, k, j = next((d, k, j) for d in range(1, n_tp + 1) for j in (1, 2)
                               for k in range(1, n_ep + 1) if d * k * j == count)
                whole = arr_a.at[pl.ds(0, d), pl.ds(0, k), pl.ds(0, j)]
            transfer(group, "fin", whole, whole).wait_send()

    only(is_edge, "edge", lambda: drain("edge"))
    only(is_mid, "mid", lambda: drain("mid"))


def flush(*refs):
    sem = refs[-1]
    copies = [pltpu.make_async_copy(refs[i], refs[9 + i], sem.at[i]) for i in range(9)]
    for copy in copies:
        copy.start()
    for copy in copies:
        copy.wait()


def fused(tokens, cotangent, routing, router_weight, gate_weight, up_weight, down_weight):
    n_ep, n_tp = lax.axis_size("ep"), lax.axis_size("tp")
    toks, width = tokens.shape
    n_exp = router_weight.shape[1]
    cap = max(2, 2 * toks * routing.shape[1] // n_exp)
    hid = gate_weight.shape[2]
    fb = width // n_tp
    two = 2 * cap
    slots = n_ep * cap
    span = width // n_ep
    results = [
        ((toks, fb), BF16),
        ((routing.shape[1], toks), F32),
        ((n_exp, span), F32),
        ((width, hid), BF16),
        ((width, hid), BF16),
        ((hid, width), BF16),
        ((2, width), F32),
        ((1, hid), F32),
        ((1, span), F32),
    ]
    vmem = pl.BlockSpec(memory_space=pltpu.VMEM)
    hbm = pl.BlockSpec(memory_space=pltpu.HBM)
    outs = pl.pallas_call(
        functools.partial(kernel, n_ep, n_tp, cap),
        out_shape=[pltpu.VMEM(shape, dtype) for shape, dtype in results],
        in_specs=[hbm] * 7,
        out_specs=[vmem] * 9,
        scratch_shapes=[
            pltpu.VMEM((routing.shape[1], toks), jnp.int32),
            pltpu.VMEM((n_exp, width), BF16),
            pltpu.VMEM((toks, width), BF16),
            pltpu.VMEM((toks, width), BF16),
            pltpu.VMEM((width, 2 * hid), BF16),
            pltpu.VMEM((hid, width), BF16),
            pltpu.VMEM((n_exp, cap, toks), BF16),
            pltpu.VMEM((n_ep // 2, 2, toks, fb), BF16),
            pltpu.VMEM((n_ep // 2, n_exp, toks), F32),
            pltpu.VMEM((2, toks, fb), BF16),
            pltpu.VMEM((2, toks, fb), BF16),
            pltpu.VMEM((n_ep // 2, 2, cap, fb), BF16),
            pltpu.VMEM((2, cap, fb), BF16),
            pltpu.VMEM((2, cap, fb), BF16),
            pltpu.VMEM((n_tp, n_ep, 2, cap, fb), BF16),
            pltpu.VMEM((n_ep, 2 * n_exp, toks), F32),
            pltpu.VMEM((n_ep // 2, 4, two, hid), F32),
            pltpu.VMEM((n_tp, n_ep, cap, fb), BF16),
            pltpu.VMEM((2, n_ep, cap, fb), BF16),
            pltpu.VMEM((n_ep, cap, fb), BF16),
            pltpu.VMEM((n_ep, cap, fb), BF16),
            pltpu.VMEM((n_ep, cap, fb), BF16),
            pltpu.VMEM((n_exp, cap, fb), BF16),
            pltpu.VMEM((slots, 2 * hid), BF16),
            pltpu.VMEM((slots, hid), BF16),
            pltpu.VMEM((n_ep // 2, 8, two), F32),
            pltpu.VMEM((n_ep // 2, 8, two), F32),
            pltpu.VMEM((n_ep // 2, 8, two), F32),
            pltpu.VMEM((n_exp, 2, 8, two), F32),
            pltpu.VMEM((two, toks), F32),
            pltpu.VMEM((2, width), F32),
            pltpu.VMEM((2, width), F32),
            pltpu.VMEM((2, width), F32),
            pltpu.VMEM((n_exp, toks), BF16),
            pltpu.VMEM((n_exp, width), F32),
            pltpu.VMEM((n_ep, n_exp, span), F32),
            pltpu.SemaphoreType.DMA((11,)),
            pltpu.SemaphoreType.DMA((SMALL + 1,)),
            pltpu.SemaphoreType.DMA((74,)),
            pltpu.SemaphoreType.REGULAR,
        ],
        compiler_params=pltpu.CompilerParams(
            collective_id=0, has_side_effects=True, vmem_limit_bytes=40 << 20
        ),
    )(*[pltpu.with_memory_space_constraint(v, pltpu.HBM)
        for v in (tokens, cotangent, routing.T, router_weight.T,
                  gate_weight[0], up_weight[0], down_weight[0])])
    outs = pl.pallas_call(
        flush,
        out_shape=[jax.ShapeDtypeStruct(shape, dtype) for shape, dtype in results],
        in_specs=[vmem] * 9,
        out_specs=[hbm] * 9,
        scratch_shapes=[pltpu.SemaphoreType.DMA((9,))],
    )(*[pltpu.with_memory_space_constraint(v, pltpu.VMEM) for v in outs])
    o_tok, o_gg, o_gr, o_gate, o_up, o_down, o_norm, o_dnorm, o_rnorm = outs
    return (o_tok, o_gg.T, o_gr.T, o_gate[None], o_up[None], o_down[None], o_norm[None],
            o_dnorm, o_rnorm[0])


def shards(tokens, cotangent, routing, router_weight, gate_weight, up_weight, down_weight):
    n_ep, n_tp = lax.axis_size("ep"), lax.axis_size("tp")
    toks, width = tokens.shape
    n_exp = router_weight.shape[1]
    cap = max(2, 2 * toks * routing.shape[1] // n_exp)
    fits = (
        n_tp == 4 and n_ep == 8 and n_ep == n_exp
        and 2 * cap == toks == 128 and gate_weight.shape[2] == 128
        and routing.shape[1] == 2 and width % (128 * 8) == 0
    )
    form = fused if fits else general
    return form(tokens, cotangent, routing, router_weight, gate_weight, up_weight, down_weight)


def solution(mesh):
    in_specs = (
        P("ep", None),
        P("ep", None),
        P("ep", None),
        P(),
        P("ep", None, "tp"),
        P("ep", None, "tp"),
        P("ep", "tp", None),
    )
    out_specs = (
        P("ep", "tp"),
        P("ep", None),
        P("ep", None),
        P("ep", None, "tp"),
        P("ep", None, "tp"),
        P("ep", "tp", None),
        P("ep", None, None),
        P("ep", "tp"),
        P("ep"),
    )
    return jax.shard_map(shards, mesh=mesh, in_specs=in_specs, out_specs=out_specs, check_vma=False)
```
